32 devices in a mesh: grp: 2 (over y), ep: 4 (over z), tp: 4 (over x, core).
Axes of the slice: x: 2, y: 2, z: 4, core: 2. Of those that a mesh axis runs over, the one named last changes fastest.
Arguments:
- out_gate: bfloat16 [1536, 4096], P(('grp', 'ep'), 'tp'), parts along dimension 0, may hold values from -6 to 6
- in_gate: bfloat16 [1536, 4096], P(('grp', 'ep'), 'tp'), parts along dimension 0, may hold values from -6 to 6
- values: bfloat16 [1536, 4096], P(('grp', 'ep'), 'tp'), parts along dimension 0, may hold values from -6 to 6
- conv_taps: float32 [3, 4096], P(None, 'tp'), may hold values from -3 to 3
- mixer_weight: bfloat16 [4096, 4096], P(None, 'tp'), may hold values from -0.09375 to 0.09375
- expert_input: bfloat16 [1536, 4096], P(('grp', 'ep', 'tp')), parts along dimension 0, may hold values from -6 to 6
- norm_gain: float32 [4096], replicated, may hold values from 0.1 to 1.9
- route_ids: int32 [1536, 2], P(('grp', 'ep')), parts along dimension 0, may hold values from 0 to 3, all different within a row; in each aligned block of 48 rows (0 to 47, 48 to 95, ...) at most 48 rows name the same one
- route_weights: float32 [1536, 2], P(('grp', 'ep')), parts along dimension 0, may hold values from 0.25 to 1.25
- gate_weight: bfloat16 [4, 4096, 1024], P('ep', None, 'tp'), may hold values from -0.09375 to 0.09375
- up_weight: bfloat16 [4, 4096, 1024], P('ep', None, 'tp'), may hold values from -0.09375 to 0.09375
- down_weight: bfloat16 [4, 1024, 4096], P('ep', None, 'tp'), may hold values from -0.1875 to 0.1875
- shared_gate: bfloat16 [4096, 512], P(None, 'tp'), may hold values from -0.09375 to 0.09375
- shared_up: bfloat16 [4096, 512], P(None, 'tp'), may hold values from -0.09375 to 0.09375
- shared_down: bfloat16 [512, 4096], P(None, 'tp'), may hold values from -0.25 to 0.25
Outputs:
- mixer_output: bfloat16 [1536, 4096], P(('grp', 'ep'), 'tp'), parts along dimension 0
- expert_output: bfloat16 [1536, 4096], P(('grp', 'ep'), 'tp'), parts along dimension 0
The draws below stay inside these ranges and needn't reach their ends.
There are 2 independent parts, one for each index of `grp`. The reference program is written for one: setup_inputs(seed, part) draws one part's arguments, and reference() takes and returns one part's arrays. A program takes and returns all parts, laid end to end along the dimension named above; an argument that names none is the same for every part. Nothing has to cross between parts.
Inputs may be any that keep to these rules, and one draw needn't show every extreme that they name: `route_ids`: the 2 entries of a row differ. In each aligned block of 48 rows (the routed tokens of one device) no expert is named by more than 48 rows, and in some block an expert is named by exactly 48 rows.
All inputs are finite; a program needn't handle non-finite values.
Results may differ from the reference program's by a relative error of at most 0.0067.
Values may be sent and summed in bfloat16 or wider, within the bound.
A program may use at most 64 MiB of HBM per device.

```python
import math
import jax
import jax.numpy as jnp
import numpy as np
from jax import lax

D = 4096
FF = 1024
SFF = 512
TOP_K = 2
TAPS = 3
TOKENS = 768
EXPERTS = 4
LANE_ROWS = 48
CAP = 48
N_EP = 4
N_TP = 4


def steps_of(key, shape, shards, least, top_value):
    gain, own = 1.0, jax.random.fold_in(key, 6)
    for dim, shards_of in shards:
        heights = jnp.exp(jax.random.uniform(jax.random.fold_in(own, dim), (shards_of,), jnp.float32, least / len(shards), top_value / len(shards)))
        gain = gain * jnp.repeat(heights, shape[dim] // shards_of).reshape([-1 if axis == dim else 1 for axis in range(len(shape))])
    return gain


def assign_block(stream_key, own, number, rows, number_of, top, bound, skew):
    ranking = jax.random.permutation(stream_key, number_of)
    heavy_load, ordinary = shares(number_of, rows * top, bound, skew, True), shares(number_of, rows * top, bound, skew, False)
    places = jnp.arange(number_of)

    def named(lengths, offset_by):
        used = int((lengths > 0).sum())
        fixed = max(1, used // 4)
        moved = fixed + (places - fixed + offset_by * (used - fixed)) % max(1, number_of - fixed)
        return jnp.zeros((number_of,), jnp.int32).at[ranking[jnp.where(places < fixed, places, moved)]].set(jnp.asarray(lengths, jnp.int32))

    lengths = jnp.where(number % 4 == 0, named(heavy_load, number // 4), named(ordinary, number - number // 4 - 1))
    mixed = jax.random.permutation(jax.random.fold_in(own, 3), number_of)
    giver, receiver = mixed[0:number_of // 2 * 2:2], mixed[1:number_of // 2 * 2:2]
    margin = jnp.minimum(lengths[giver] - 1, bound - lengths[receiver]) // 2
    margin = jnp.where((giver == ranking[0]) | (receiver == ranking[0]) | (lengths[receiver] == 0), 0, jnp.maximum(margin, 0))
    moved = jax.random.randint(jax.random.fold_in(own, 4), (number_of // 2,), 0, 1 << 20) % (margin + 1)
    lengths = lengths.at[giver].add(-moved).at[receiver].add(moved)
    labels = jnp.searchsorted(jnp.cumsum(lengths), jnp.arange(rows * top), side="right").astype(jnp.int32)
    listing = labels.reshape(top, rows).T
    listing = listing[jax.random.permutation(jax.random.fold_in(own, 1), rows)]
    offset_by = jax.random.randint(jax.random.fold_in(own, 2), (rows, 1), 0, top)
    return jnp.take_along_axis(listing, (jnp.arange(top)[None, :] + offset_by) % top, axis=1)


def shares(count, total, reach, lean, full):
    weights = [(1 << 20) // math.isqrt(grade ** lean) + 1 for grade in range(1, count + 1)]
    largest = reach if full else min(reach, max(-(-total // count), total * weights[0] // sum(weights)))
    least = 1 if total - largest >= count - 1 else 0
    counts, spare = [largest] + [least] * (count - 1), total - largest - least * (count - 1)
    while spare > 0:
        movable = [i for i in range(1, count) if counts[i] < largest] or [i for i in range(1, count) if counts[i] < reach]
        whole, budget = sum([weights[i] for i in movable]), spare
        for i in movable:
            extra = min(reach - counts[i], max(1, budget * weights[i] // whole), spare)
            counts[i] = counts[i] + extra
            spare = spare - extra
    return np.array(counts)


def bell_draw(key, extent, deviation, most, pieces=(), kind=jnp.bfloat16):
    values = deviation * jax.random.normal(key, extent, jnp.float32)
    if pieces:
        values = values * steps_of(key, extent, pieces, -0.22, 0.18)
    return jnp.clip(values, -most, most).astype(kind)


def setup_inputs(seed: int = 0, part: int = 0) -> dict:
    seeds = jax.random.split(jax.random.key(seed), 16)
    part_keys = jax.random.split(jax.random.fold_in(seeds[15], part), 16)
    out_gate = bell_draw(part_keys[0], (TOKENS, D), 1.0, 6.0, ((0, 4), (1, 4)))
    in_gate = bell_draw(part_keys[1], (TOKENS, D), 1.0, 6.0, ((0, 4), (1, 4)))
    values = bell_draw(part_keys[2], (TOKENS, D), 1.0, 6.0, ((0, 4), (1, 4)))
    conv_taps = bell_draw(seeds[3], (TAPS, D), 0.6, 3.0, ((1, 4),), jnp.float32)
    mixer_weight = bell_draw(seeds[4], (D, D), D ** -0.5, 0.09375, ((1, 4),))
    expert_input = bell_draw(part_keys[5], (TOKENS, D), 1.0, 6.0, ((0, 16),))
    norm_gain = jnp.clip(1.0 + 0.18 * jax.random.normal(seeds[6], (D,), jnp.float32), 0.1, 1.9)
    route_ids_keys = jax.random.split(jax.random.fold_in(part_keys[7], 1), TOKENS // LANE_ROWS)
    route_ids_turns = jax.random.permutation(jax.random.fold_in(part_keys[7], 3), TOKENS // LANE_ROWS)
    route_ids = jax.vmap(lambda own, number: assign_block(jax.random.fold_in(part_keys[7], 2), own, number, LANE_ROWS, EXPERTS, TOP_K, CAP, 2))(route_ids_keys, route_ids_turns).reshape((TOKENS, TOP_K))
    route_weights = jnp.clip(0.25 + 1.0 * jax.random.uniform(part_keys[8], (TOKENS, TOP_K), jnp.float32) ** steps_of(part_keys[8], (TOKENS, TOP_K), ((0, 4),), -0.2, 0.2), 0.25, 1.25)
    gate_weight = bell_draw(seeds[9], (EXPERTS, D, FF), D ** -0.5, 0.09375, ((0, 4), (2, 4)))
    up_weight = bell_draw(seeds[10], (EXPERTS, D, FF), D ** -0.5, 0.09375, ((0, 4), (2, 4)))
    down_weight = bell_draw(seeds[11], (EXPERTS, FF, D), FF ** -0.5, 0.1875, ((0, 4), (2, 4)))
    shared_gate = bell_draw(seeds[12], (D, SFF), D ** -0.5, 0.09375, ((1, 4),))
    shared_up = bell_draw(seeds[13], (D, SFF), D ** -0.5, 0.09375, ((1, 4),))
    shared_down = bell_draw(seeds[14], (SFF, D), SFF ** -0.5, 0.25, ((1, 4),))
    return dict(out_gate=out_gate, in_gate=in_gate, values=values, conv_taps=conv_taps, mixer_weight=mixer_weight, expert_input=expert_input, norm_gain=norm_gain, route_ids=route_ids, route_weights=route_weights, gate_weight=gate_weight, up_weight=up_weight, down_weight=down_weight, shared_gate=shared_gate, shared_up=shared_up, shared_down=shared_down)


norm_floor = 0.5

def layer_norm(tokens, norm_gain):
    widened = tokens.astype(jnp.float32)
    centred = widened - lax.optimization_barrier(jnp.mean(widened, axis=-1, keepdims=True))
    spread = lax.optimization_barrier(jnp.mean(centred * centred, axis=-1, keepdims=True))
    return (centred * lax.rsqrt(spread + norm_floor) * norm_gain).astype(jnp.bfloat16)

def expert_hidden(inputs, gate_part, up_part):
    gate_value = jnp.dot(inputs, gate_part, preferred_element_type=jnp.float32)
    up_value = jnp.dot(inputs, up_part, preferred_element_type=jnp.float32)
    return (jax.nn.silu(gate_value) * up_value).astype(jnp.bfloat16)

def reference(out_gate, in_gate, values, conv_taps, mixer_weight, expert_input, norm_gain, route_ids, route_weights, gate_weight, up_weight, down_weight, shared_gate, shared_up, shared_down):
    gated_values = (in_gate.astype(jnp.float32) * values.astype(jnp.float32)).astype(jnp.bfloat16)
    extended = jnp.concatenate([jnp.zeros((TAPS - 1, D), jnp.bfloat16), gated_values], axis=0).astype(jnp.float32)
    conv_state = conv_taps[0] * extended[:-2] + conv_taps[1] * extended[1:-1] + conv_taps[2] * extended[2:]
    mixed_rows = (out_gate.astype(jnp.float32) * conv_state).astype(jnp.bfloat16)
    mixer_output = jnp.dot(mixed_rows, mixer_weight, preferred_element_type=jnp.float32).astype(jnp.bfloat16)
    normed_rows = layer_norm(expert_input, norm_gain)
    buffer_len = N_EP * N_TP * CAP
    flat_ids = route_ids.reshape(-1).astype(jnp.int32)
    onehot = (flat_ids[:, None] == jnp.arange(EXPERTS, dtype=jnp.int32)[None, :]).astype(jnp.int32)
    slot_index = lax.optimization_barrier(jnp.sum((jnp.cumsum(onehot, axis=0) - onehot) * onehot, axis=1)).astype(jnp.int32)
    positions = flat_ids * buffer_len + slot_index
    owners = jnp.full((EXPERTS * buffer_len,), TOKENS, jnp.int32)
    owners = owners.at[positions].set(jnp.arange(TOKENS * TOP_K, dtype=jnp.int32) // TOP_K)

    def run_expert(operands):
        owner_rows, gate_part, up_part, down_part = operands
        picked = jnp.take(normed_rows, owner_rows, axis=0, mode='fill', fill_value=0)
        hidden = expert_hidden(picked, gate_part, up_part)
        return jnp.dot(hidden, down_part, preferred_element_type=jnp.float32).astype(jnp.bfloat16)
    results = lax.map(run_expert, (owners.reshape(EXPERTS, buffer_len), gate_weight, up_weight, down_weight))
    picked = jnp.take(results.reshape(EXPERTS * buffer_len, D), positions, axis=0).astype(jnp.float32)
    picked = picked.reshape(TOKENS, TOP_K, D)
    shared_hidden = expert_hidden(normed_rows, shared_gate, shared_up)
    shared_result = jnp.dot(shared_hidden, shared_down, preferred_element_type=jnp.float32)
    expert_output = (shared_result + lax.optimization_barrier(jnp.sum(route_weights[:, :, None] * picked, axis=1))).astype(jnp.bfloat16)
    return (mixer_output, expert_output)
```

```python
import functools

import jax
import jax.numpy as jnp
from jax import lax
from jax.experimental import pallas as pl
from jax.experimental.pallas import tpu as pltpu
from jax.sharding import PartitionSpec as P

MESH = pl.DeviceIdType.MESH
CORES = 2
TILE = 256
PIECE = 16
CHUNKS = 4
ROLES = 2

norm_floor = 0.5


def shifted(value, axis, steps):
    count = lax.axis_size(axis)
    leading, last = (max(0, -steps), min(count, count - steps))
    return lax.ppermute(value, axis, [(source, source + steps) for source in range(leading, last)])


def layer_norm(tokens, norm_gain):
    widened = tokens.astype(jnp.float32)
    centred = widened - jnp.mean(widened, axis=-1, keepdims=True)
    spread = jnp.mean(centred * centred, axis=-1, keepdims=True)
    return (centred * lax.rsqrt(spread + norm_floor) * norm_gain).astype(jnp.bfloat16)


def expert_hidden(inputs, gate_part, up_part):
    gate_value = jnp.dot(inputs, gate_part, preferred_element_type=jnp.float32)
    up_value = jnp.dot(inputs, up_part, preferred_element_type=jnp.float32)
    return (jax.nn.silu(gate_value) * up_value).astype(jnp.bfloat16)


def slot_ranks(route_ids, experts, lanes):
    tok_count, top_count = route_ids.shape
    grouped = route_ids.reshape(lanes, tok_count // lanes * top_count)
    onehot = (grouped[:, :, None] == jnp.arange(experts, dtype=jnp.int32)[None, None, :]).astype(
        jnp.int32
    )
    before = jnp.cumsum(onehot, axis=1) - onehot
    return jnp.sum(before * onehot, axis=2).reshape(tok_count, top_count)


def plain(
    out_gate,
    in_gate,
    values,
    conv_taps,
    mixer_weight,
    expert_input,
    norm_gain,
    route_ids,
    route_weights,
    gate_weight,
    up_weight,
    down_weight,
    shared_gate,
    shared_up,
    shared_down,
):
    experts = lax.axis_size("ep")
    lanes = lax.axis_size("tp")
    lane_rows = expert_input.shape[0]
    width = expert_input.shape[1]
    tok_count, top_count = route_ids.shape
    capacity = (2 * lane_rows * top_count + experts - 1) // experts
    gated_values = (in_gate.astype(jnp.float32) * values.astype(jnp.float32)).astype(jnp.bfloat16)
    previous = shifted(gated_values[-2:], "ep", 1)
    extended = jnp.concatenate([previous, gated_values], axis=0).astype(jnp.float32)
    conv_state = (
        conv_taps[0] * extended[:-2] + conv_taps[1] * extended[1:-1] + conv_taps[2] * extended[2:]
    )
    mixed_rows = (out_gate.astype(jnp.float32) * conv_state).astype(jnp.bfloat16)
    normed_own = layer_norm(expert_input, norm_gain)
    mixed_whole, normed_rows = (
        lax.all_gather(mixed_rows, "tp", axis=1, tiled=True),
        lax.all_gather(normed_own, "tp", axis=0, tiled=True),
    )
    mixer_output = jnp.dot(mixed_whole, mixer_weight, preferred_element_type=jnp.float32).astype(
        jnp.bfloat16
    )
    shared_part = expert_hidden(normed_rows, shared_gate, shared_up)
    slot_index = slot_ranks(route_ids, experts, lanes)
    lane_of_row = (jnp.arange(tok_count, dtype=jnp.int32) // lane_rows)[:, None]
    positions = (route_ids * lanes + lane_of_row) * capacity + slot_index
    lane_index = lax.axis_index("tp")
    lane_ids = lax.dynamic_slice_in_dim(route_ids, lane_index * lane_rows, lane_rows, 0)
    lane_slots = lax.dynamic_slice_in_dim(slot_index, lane_index * lane_rows, lane_rows, 0)
    lane_places = lane_ids * capacity + lane_slots
    local_rows = jnp.broadcast_to(jnp.arange(lane_rows, dtype=jnp.int32)[:, None], lane_ids.shape)
    owners = jnp.full((experts * capacity,), lane_rows, jnp.int32)
    owners = owners.at[lane_places.reshape(-1)].set(local_rows.reshape(-1))
    outgoing = jnp.take(normed_own, owners, axis=0, mode="fill", fill_value=0)
    arrived = lax.all_to_all(
        outgoing.reshape(experts, capacity, width), "ep", split_axis=0, concat_axis=0, tiled=True
    )
    segment = lax.all_gather(arrived[None], "tp", axis=0, tiled=True)
    hidden_rows = expert_hidden(segment.reshape(-1, width), gate_weight[0], up_weight[0])
    spread_hidden = hidden_rows.reshape(segment.shape[:-1] + (hidden_rows.shape[-1],))
    routed_hidden = jnp.swapaxes(spread_hidden, 0, 1).reshape(-1, spread_hidden.shape[-1])
    routed_whole, shared_whole = (
        lax.all_gather(routed_hidden, "tp", axis=1, tiled=True),
        lax.all_gather(shared_part, "tp", axis=1, tiled=True),
    )
    routed_result = jnp.dot(
        routed_whole, down_weight[0], preferred_element_type=jnp.float32
    ).astype(jnp.bfloat16)
    out_cols = routed_result.shape[-1]
    returned = lax.all_to_all(
        routed_result.reshape(experts, lanes * capacity, out_cols),
        "ep",
        split_axis=0,
        concat_axis=0,
        tiled=True,
    )
    shared_result = jnp.dot(shared_whole, shared_down, preferred_element_type=jnp.float32)
    picked = jnp.take(
        returned.reshape(experts * lanes * capacity, out_cols), positions.reshape(-1), axis=0
    )
    picked = picked.astype(jnp.float32).reshape(tok_count, top_count, out_cols)
    expert_output = (shared_result + jnp.sum(route_weights[:, :, None] * picked, axis=1)).astype(
        jnp.bfloat16
    )
    return (mixer_output, expert_output)


def silu_product(gate_value, up_value):
    return (gate_value * (1.0 / (1.0 + jnp.exp(-gate_value))) * up_value).astype(jnp.bfloat16)


def dot32(left, right):
    return jnp.dot(left, right, preferred_element_type=jnp.float32)


def kernel(
    n_ep,
    n_tp,
    ids,
    rw,
    og_h,
    ig_h,
    va_h,
    taps_h,
    mw_h,
    ei_h,
    ng_h,
    gw_h,
    uw_h,
    dw_h,
    sg_h,
    su_h,
    sd_h,
    mix_out,
    exp_out,
    og,
    ig,
    va,
    taps,
    mw,
    ei,
    ng,
    gw,
    uw,
    dw,
    sg,
    su,
    sd,
    tok,
    hid,
    shd,
    mixed,
    gated,
    halo,
    res,
    pin,
    acc,
    wts,
    ld,
    z_send,
    z_recv,
    x_send,
    x_recv,
    p_send,
    p_recv,
    r_send,
    r_recv,
    w_send,
    w_recv,
    h_sem,
):
    e = lax.axis_index("ep")
    t = lax.axis_index("tp")
    n_x = n_tp // CORES
    partner = t + 1 - 2 * (t % CORES)
    lane_rows, width = ei.shape
    rows, chans = og.shape

    loads = {}
    for number, (name, src, dst) in enumerate(
        (
            ("ei", ei_h, ei),
            ("ng", ng_h, ng),
            ("ig", ig_h, ig),
            ("va", va_h, va),
            ("og", og_h, og),
            ("taps", taps_h, taps),
            ("gw", gw_h, gw),
            ("uw", uw_h, uw),
            ("sg", sg_h, sg),
            ("su", su_h, su),
            ("dw", dw_h, dw),
            ("sd", sd_h, sd),
            ("mw", mw_h, mw),
        )
    ):
        loads[name] = pltpu.make_async_copy(src, dst, ld.at[number])
        loads[name].start()

    barrier = pltpu.get_barrier_semaphore()
    greeted = [{"ep": (e + d) % n_ep, "tp": t} for d in range(1, n_ep)]
    greeted += [{"ep": e, "tp": (t + CORES * d) % n_tp} for d in range(1, n_x)]
    greeted += [{"ep": e, "tp": partner}]
    for peer in greeted:
        pl.semaphore_signal(barrier, inc=1, device_id=peer, device_id_type=MESH)

    def remote(src, dst, send, recv, ep, tp):
        return pltpu.make_async_remote_copy(
            src_ref=src,
            dst_ref=dst,
            send_sem=send,
            recv_sem=recv,
            device_id={"ep": ep, "tp": tp},
            device_id_type=MESH,
        )

    def cross(slot, g, d, lane):
        return remote(
            slot(lane), slot(lane), x_send.at[g, d - 1], x_recv.at[g, d - 1],
            e, (t + CORES * d) % n_tp,
        )

    def across(slot, g, d, lane):
        return remote(slot(lane), slot(lane), p_send.at[g, d], p_recv.at[g, d], e, partner)

    def from_x(d):
        return (t + n_tp - CORES * d) % n_tp

    def from_partner(d):
        return (partner + n_tp - CORES * d) % n_tp

    def gather_start(slot, g):
        for d in range(1, n_x):
            cross(slot, g, d, t).start()
        across(slot, g, 0, t).start()

    def gather_forward(slot, g):
        for d in range(1, n_x):
            cross(slot, g, d, from_x(d)).wait_recv()
            across(slot, g, d, from_x(d)).start()

    def gather_finish(slot, g):
        for d in range(n_x):
            across(slot, g, d, from_partner(d)).wait_recv()

    def gather_drain(slot, g):
        for d in range(1, n_x):
            cross(slot, g, d, t).wait_send()
            across(slot, g, d, from_x(d)).wait_send()
        across(slot, g, 0, t).wait_send()

    pieces = lane_rows // PIECE
    first_hidden = n_ep * pieces
    shared_g = first_hidden + n_ep
    mixed_g = shared_g + 1

    def tok_slot(j, q):
        return lambda lane: tok.at[j, lane, q]

    def hid_slot(j):
        return lambda lane: hid.at[j, lane]

    def shd_slot(lane):
        return shd.at[lane]

    def mixed_slot(lane):
        return mixed.at[lane]

    last = n_ep - 1
    flipped = e > last - e
    inner = (e > 0) & (e < last)
    up = jnp.where(flipped, e - 1, e + 1)
    down = jnp.clip(jnp.where(flipped, e + 1, e - 1), 0, last)

    def block_at(m):
        return jnp.where(flipped, last - m, m)

    def z_copy(side, d, j, q):
        block = tok.at[j, from_x(d), q]
        return remote(block, block, z_send.at[side, d, j, q], z_recv.at[d, j, q],
                      up if side == 0 else down, t)

    def arrive(m, q, onward=None, crosses=True):
        j = block_at(m)
        z_copy(0, 0, j, q).wait_recv()
        if onward is not None:
            z_copy(onward, 0, j, q).start()
        if crosses:
            for d in range(1, n_x):
                cross(tok_slot(j, q), j * pieces + q, d, t).start()
        across(tok_slot(j, q), j * pieces + q, 0, t).start()

    def arrive_beside(m, q):
        j = block_at(m)
        for d in range(1, n_x):
            z_copy(0, d, j, q).wait_recv()
            across(tok_slot(j, q), j * pieces + q, d, from_x(d)).start()

    def crossed(m, q, onward=None):
        j = block_at(m)
        for d in range(1, n_x):
            cross(tok_slot(j, q), j * pieces + q, d, from_x(d)).wait_recv()
            if onward is not None:
                z_copy(onward, d, j, q).start()
            across(tok_slot(j, q), j * pieces + q, d, from_x(d)).start()

    def own_onward(side, d, q):
        z_copy(side, d, e, q).start()

    piece = rows // CHUNKS

    def span(c):
        return pl.ds(pl.multiple_of(c * piece, 16), piece)

    def hop(j, c):
        after = jnp.clip(jnp.where(j > e, e + 1, e - 1), 0, last)
        slot = jnp.where((j < e) & (after == j), n_ep, j)
        return remote(res.at[j, span(c)], pin.at[slot, span(c)],
                      r_send.at[j, c], r_recv.at[slot, c], after, t)

    def hop_arrives(slot, c):
        remote(res.at[0, span(c)], pin.at[slot, span(c)], r_send.at[0, c], r_recv.at[slot, c],
               jnp.clip(e + 1, 0, last), t).wait_recv()

    def relay(m, c):
        j = block_at(m)
        hop_arrives(j, c)
        total = res[j, span(c), :].astype(jnp.float32) + pin[j, span(c), :].astype(jnp.float32)
        res[j, span(c), :] = total.astype(jnp.bfloat16)
        hop(j, c).start()

    def weights_to(d):
        return remote(wts.at[e], wts.at[e], w_send.at[d - 1], w_recv.at[e], (e + d) % n_ep, t)

    def weight_column(j):
        held = wts[j]
        mine = jnp.where(lax.broadcasted_iota(jnp.int32, held.shape, 0) == e, held, 0.0)
        line = jnp.sum(mine, axis=0, keepdims=True)
        shape = (rows, held.shape[1])
        same = lax.broadcasted_iota(jnp.int32, shape, 0) == lax.broadcasted_iota(jnp.int32, shape, 1)
        return jnp.sum(jnp.where(same, line, 0.0), axis=1, keepdims=True)

    loads["ei"].wait()
    loads["ng"].wait()

    def norm_rows(r, _):
        at = pl.ds(pl.multiple_of(r * PIECE, PIECE), PIECE)
        widened = ei[at, :].astype(jnp.float32)
        centred = widened - jnp.mean(widened, axis=-1, keepdims=True)
        spread_of = jnp.mean(centred * centred, axis=-1, keepdims=True)
        normed = centred * lax.rsqrt(spread_of + norm_floor) * ng[...]
        tok[e, t, r] = normed.astype(jnp.bfloat16)
        return 0

    lax.fori_loop(0, pieces, norm_rows, 0)
    with jax.named_scope("barrier"):
        pl.semaphore_wait(barrier, len(greeted))

    for q in range(pieces):
        own_onward(0, 0, q)

        if q < pieces - 1:

            @pl.when(inner)
            def _():
                own_onward(1, 0, q)

        for d in range(1, n_x):
            cross(tok_slot(e, q), e * pieces + q, d, t).start()
        across(tok_slot(e, q), e * pieces + q, 0, t).start()

    place = lax.broadcasted_iota(jnp.int32, (wts.shape[1], rows), 0)
    dense = jnp.zeros(place.shape, jnp.float32)
    for k in range(ids.shape[0]):
        dense += jnp.where(ids[k : k + 1, :] == place, rw[k : k + 1, :], 0.0)
    wts[e] = jnp.zeros(wts.shape[1:], jnp.float32)
    wts[e, :, 0:rows] = dense
    for d in range(1, n_ep):
        weights_to(d).start()

    loads["ig"].wait()
    loads["va"].wait()

    def gate_cols(c, _):
        at = pl.ds(pl.multiple_of(c * 128, 128), 128)
        gated[:, at] = (ig[:, at].astype(jnp.float32) * va[:, at].astype(jnp.float32)).astype(
            jnp.bfloat16
        )
        return 0

    lax.fori_loop(0, chans // 128, gate_cols, 0)

    def halo_copy():
        return remote(gated.at[pl.ds(rows - 16, 16)], halo, h_sem.at[0], h_sem.at[1],
                      jnp.minimum(e + 1, last), t)

    @pl.when(e < last)
    def _():
        halo_copy().start()

    @pl.when(e == 0)
    def _():
        halo[...] = jnp.zeros_like(halo)

    for here, slot in ((e > 0, e), (e < last, n_ep)):

        @pl.when(~here)
        def _():
            pin[slot] = jnp.zeros(pin.shape[1:], pin.dtype)

    def mix_cols(c, _):
        at = pl.ds(pl.multiple_of(c * 128, 128), 128)
        now = gated[:, at].astype(jnp.float32)
        before = halo[:, at].astype(jnp.float32)
        place = lax.broadcasted_iota(jnp.int32, now.shape, 0)
        one = jnp.where(place == 0, before[15:16], pltpu.roll(now, 1, 0))
        two = jnp.where(
            place == 0, before[14:15], jnp.where(place == 1, before[15:16], pltpu.roll(now, 2, 0))
        )
        state = taps[0:1, at] * two + taps[1:2, at] * one + taps[2:3, at] * now
        mixed[t, :, at] = (og[:, at].astype(jnp.float32) * state).astype(jnp.bfloat16)
        return 0

    def end_tokens():
        for q in range(pieces):
            if q < pieces - 1:
                arrive(1, q, crosses=False)
            crossed(0, q, onward=0)
        for q in range(pieces):
            arrive(2, q)
            if q:
                crossed(2, q - 1)
        arrive(3, 0)
        crossed(2, pieces - 1)

    def end_more():
        for q in range(1, pieces):
            arrive(3, q)
            crossed(3, q - 1)
        arrive(1, pieces - 1, crosses=False)

    def end_last():
        crossed(3, pieces - 1)

    def end_beside():
        for q in range(pieces):
            arrive_beside(1, q)

    def inner_tokens():
        for q in range(pieces):
            arrive(0, q, onward=0, crosses=False)
            arrive(2, q, onward=1)
            crossed(1, q)
        for q in range(pieces):
            arrive(3, q, onward=1)
            arrive_beside(0, q)
            crossed(2, q)
        own_onward(1, 0, pieces - 1)
        for d in range(1, n_x):
            for q in range(pieces):
                own_onward(1, d, q)

    def inner_more():
        for q in range(pieces):
            crossed(3, q)

    def relays(m, chunks):
        for c in chunks:
            relay(m, c)

    half = CHUNKS // 2
    early, late = range(half), range(half, CHUNKS)
    steps = 7
    gates = ((2, 3, 1, 0), (2, 0, 3, 1))
    downs = ((-1, 2, -1, 3, 1, 0, -1), (-1, -1, -1, 2, 3, 0, 1))
    before_down = (
        {1: end_more},
        {5: lambda: relays(2, early), 6: lambda: relays(2, late)},
    )
    before_gate = (
        {0: end_tokens, 1: end_last, 2: end_beside},
        {0: inner_tokens, 2: inner_more},
    )

    def table(pair, s):
        found = jnp.int32(-1)
        for k, (end_m, inner_m) in enumerate(zip(*pair)):
            found = jnp.where(s == k, jnp.where(inner, inner_m, end_m), found)
        return found

    def due(pair, s):
        for part, here in zip(pair, (~inner, inner)):
            for k, what in part.items():

                @pl.when(here & (s == k))
                def _():
                    what()

    def down_block(j):
        part = hid.shape[-1]
        with jax.named_scope("hid_wait"):
            gather_forward(hid_slot(j), first_hidden + j)
            gather_finish(hid_slot(j), first_hidden + j)

            @pl.when(j != e)
            def _():
                remote(wts.at[e], wts.at[j], w_send.at[0], w_recv.at[j], j, t).wait_recv()

        with jax.named_scope("down"):
            weight = weight_column(j)
            for c in range(chans // TILE):
                at = slice(c * TILE, (c + 1) * TILE)
                total = dot32(hid[j, 0], dw[0:part, at])
                for lane in range(1, n_tp):
                    total += dot32(hid[j, lane], dw[lane * part : (lane + 1) * part, at])
                res[j, :, at] = (weight * total).astype(jnp.bfloat16)

        @pl.when((j != e) & ~inner)
        def _():
            for c in range(CHUNKS):
                hop(j, c).start()

    def gate_block(j, s):
        with jax.named_scope("gate_wait"):
            for q in range(pieces):
                gather_finish(tok_slot(j, q), j * pieces + q)

            @pl.when(s == 0)
            def _():
                for name in ("gw", "uw", "sg", "su", "dw"):
                    loads[name].wait()

        with jax.named_scope("gate"):
            block = tok[j].reshape(rows, width)
            hid[j, t] = silu_product(dot32(block, gw[...]), dot32(block, uw[...]))
            gather_start(hid_slot(j), first_hidden + j)

    def step(s, _):
        with jax.named_scope("pre_down"):
            due(before_down, s)
        down_m = table(downs, s)

        @pl.when(down_m >= 0)
        def _():
            down_block(block_at(down_m))

        with jax.named_scope("pre_gate"):
            due(before_gate, s)

        @pl.when(s < n_ep)
        def _():
            gate_block(block_at(table(gates, s)), s)

        @pl.when(s == n_ep - 1)
        def _():
            with jax.named_scope("shared"):
                block = tok[e].reshape(rows, width)
                shd[t] = silu_product(dot32(block, sg[...]), dot32(block, su[...]))
                gather_start(shd_slot, shared_g)
            with jax.named_scope("mix"):
                loads["og"].wait()
                loads["taps"].wait()

                @pl.when(e > 0)
                def _():
                    halo_copy().wait_recv()

                lax.fori_loop(0, chans // 128, mix_cols, 0)
                gather_start(mixed_slot, mixed_g)

        return 0

    lax.fori_loop(0, steps, step, 0)

    with jax.named_scope("acc"):
        gather_forward(shd_slot, shared_g)

        @pl.when(inner)
        def _():
            relay(3, 0)

        loads["sd"].wait()
        gather_finish(shd_slot, shared_g)

        def shared_cols(c, _):
            at = pl.ds(pl.multiple_of(c * TILE, TILE), TILE)
            part = shd.shape[-1]
            total = dot32(shd[0], sd[0:part, at])
            for lane in range(1, n_tp):
                total += dot32(shd[lane], sd[lane * part : (lane + 1) * part, at])
            acc[:, at] = total + res[e, :, at].astype(jnp.float32)
            return 0

        lax.fori_loop(0, chans // TILE, shared_cols, 0)

    with jax.named_scope("mixed_wait"):
        @pl.when(inner)
        def _():
            relay(3, 1)

        loads["mw"].wait()
        gather_forward(mixed_slot, mixed_g)
        gather_finish(mixed_slot, mixed_g)

    tiles = chans // TILE
    rest = [(3, c) for c in range(2, CHUNKS)]
    back = [(0, c) for c in range(CHUNKS)]
    waves = []
    while rest or back:
        waves.append([pop.pop(0) for pop in (rest, back) if pop])

    def mixer_cols(c, _):
        with jax.named_scope("relay"):
            for k in range(tiles):
                share = [one for w in range(k, len(waves), tiles) for one in waves[w]]

                @pl.when(inner & (c == k))
                def _():
                    for m, chunk in share:
                        relay(m, chunk)

        with jax.named_scope("mixer"):
            at = pl.ds(pl.multiple_of(c * TILE, TILE), TILE)
            total = dot32(mixed[0], mw[0:chans, at])
            for lane in range(1, n_tp):
                total += dot32(mixed[lane], mw[lane * chans : (lane + 1) * chans, at])
            mix_out[:, at] = total.astype(jnp.bfloat16)
        return 0

    lax.fori_loop(0, tiles, mixer_cols, 0)

    def combine(c, _):
        with jax.named_scope("final_wait"):
            for here, slot in ((e > 0, e), (e < last, n_ep)):

                @pl.when(here)
                def _():
                    hop_arrives(slot, c)

        total = acc[span(c), :]
        for found in (pin[e, span(c), :], pin[n_ep, span(c), :]):
            total += found.astype(jnp.float32)
        exp_out[span(c), :] = total.astype(jnp.bfloat16)
        return 0

    lax.fori_loop(0, CHUNKS, combine, 0)

    @pl.when(e < last)
    def _():
        halo_copy().wait_send()

    with jax.named_scope("drain"):
        for q in range(pieces):
            for side, d, m in ((0, 0, None),):
                z_copy(side, d, e, q).wait_send()

            @pl.when(~inner)
            def _():
                for d in range(1, n_x):
                    z_copy(0, d, e, q).wait_send()

            @pl.when(inner)
            def _():
                for d in range(n_x):
                    z_copy(1, d, e, q).wait_send()
                z_copy(0, 0, block_at(0), q).wait_send()
                for m in (2, 3):
                    z_copy(1, 0, block_at(m), q).wait_send()

        beside = jnp.where(inner, block_at(0), block_at(1))

        def drain(j, _):
            for q in range(pieces):
                g = j * pieces + q
                across(tok_slot(j, q), g, 0, t).wait_send()
                for d in range(1, n_x):

                    @pl.when(j != beside)
                    def _():
                        cross(tok_slot(j, q), g, d, t).wait_send()

                    across(tok_slot(j, q), g, d, from_x(d)).wait_send()
            gather_drain(hid_slot(j), first_hidden + j)

            @pl.when(j != e)
            def _():
                for c in range(CHUNKS):
                    hop(j, c).wait_send()

            return 0

        lax.fori_loop(0, n_ep, drain, 0)
        for d in range(1, n_ep):
            weights_to(d).wait_send()
        gather_drain(shd_slot, shared_g)
        gather_drain(mixed_slot, mixed_g)


def joined(n_ep, n_tp, *args):
    (og, ig, va, taps, mw, ei, ng, ids, rw, gw, uw, dw, sg, su, sd) = args
    gw, uw, dw, ng = gw[0], uw[0], dw[0], ng[None]
    bf, f32 = jnp.bfloat16, jnp.float32
    rows, chans = og.shape
    lane_rows, width = ei.shape
    n_x = n_tp // CORES
    pieces = lane_rows // PIECE
    sems = n_ep * pieces + n_ep + 2
    big = (og, ig, va, taps, mw, ei, ng, gw, uw, dw, sg, su, sd)
    out = jax.ShapeDtypeStruct((rows, chans), bf)
    vmem = pl.BlockSpec(memory_space=pltpu.VMEM)
    dma = pltpu.SemaphoreType.DMA
    return pl.pallas_call(
        functools.partial(kernel, n_ep, n_tp),
        out_shape=(out, out),
        in_specs=[vmem, vmem] + [pl.BlockSpec(memory_space=pl.ANY)] * len(big),
        out_specs=(vmem, vmem),
        scratch_shapes=[pltpu.VMEM(a.shape, a.dtype) for a in big]
        + [
            pltpu.VMEM((n_ep, n_tp, pieces, PIECE, width), bf),
            pltpu.VMEM((n_ep, n_tp, rows, gw.shape[-1]), bf),
            pltpu.VMEM((n_tp, rows, sg.shape[-1]), bf),
            pltpu.VMEM((n_tp, rows, chans), bf),
            pltpu.VMEM((rows, chans), bf),
            pltpu.VMEM((16, chans), bf),
            pltpu.VMEM((n_ep, rows, chans), bf),
            pltpu.VMEM((n_ep + 1, rows, chans), bf),
            pltpu.VMEM((rows, chans), f32),
            pltpu.VMEM((n_ep, -(-n_ep // 8) * 8, -(-rows // 128) * 128), f32),
            dma((len(big),)),
            dma((2, n_x, n_ep, pieces)),
            dma((n_x, n_ep, pieces)),
            dma((sems, max(1, n_x - 1))),
            dma((sems, max(1, n_x - 1))),
            dma((sems, n_x)),
            dma((sems, n_x)),
            dma((n_ep, CHUNKS)),
            dma((n_ep + 1, CHUNKS)),
            dma((n_ep,)),
            dma((n_ep,)),
            dma((2,)),
        ],
        compiler_params=pltpu.CompilerParams(
            collective_id=0, has_side_effects=True, vmem_limit_bytes=60 * 1024 * 1024
        ),
    )(ids.T, rw.T, *big)


def local(*args):
    n_ep, n_tp = lax.axis_size("ep"), lax.axis_size("tp")
    chans, lane_rows = args[0].shape[1], args[5].shape[0]
    aligned = (
        n_tp % CORES == 0
        and n_ep == 2 * ROLES
        and lane_rows % PIECE == 0
        and lane_rows * n_tp == args[0].shape[0]
        and chans % TILE == 0
        and args[0].shape[0] % (16 * CHUNKS) == 0
        and args[9].shape[2] % 128 == 0
        and args[12].shape[1] % 128 == 0
    )
    return joined(n_ep, n_tp, *args) if aligned else plain(*args)


def solution(mesh):
    placed = (
        P(("grp", "ep"), "tp"),
        P(("grp", "ep"), "tp"),
        P(("grp", "ep"), "tp"),
        P(None, "tp"),
        P(None, "tp"),
        P(("grp", "ep", "tp"), None),
        P(),
        P(("grp", "ep"), None),
        P(("grp", "ep"), None),
        P("ep", None, "tp"),
        P("ep", None, "tp"),
        P("ep", None, "tp"),
        P(None, "tp"),
        P(None, "tp"),
        P(None, "tp"),
    )
    return jax.shard_map(
        local,
        mesh=mesh,
        in_specs=placed,
        out_specs=(P(("grp", "ep"), "tp"), P(("grp", "ep"), "tp")),
        check_vma=False,
    )
```

```python
import functools

import jax
import jax.numpy as jnp
from jax import lax
from jax.experimental import pallas as pl
from jax.experimental.pallas import tpu as pltpu
from jax.sharding import PartitionSpec as P

MESH = pl.DeviceIdType.MESH
CORES = 2
TILE = 256
PIECE = 16
CHUNKS = 4
ROLES = 2
STEPS = 3
SUB = 1

END_PLAN = dict(
    gates=("20", "21", "22", "30", "31", "32", "10", "11", "12", "--", "--", "--"),
    downs=("--", "--", "--", "20", "21", "22", "30", "31", "32", "10", "11", "12"),
    before_down={
    },
    before_gate={
        0: ("N10", "O00", "N11", "O01", "X00", "M00", "O02", "A20", "D00", "E00", "A21", "S00", "B20"),
        1: ("A22", "W00", "B21"),
        2: ("A30", "B22", "A31", "H20"),
        3: ("A32", "B30", "H21"),
        4: ("N12", "B31", "H22"),
        5: ("Z10", "B32", "H30"),
        6: ("H31",),
        7: ("Z11", "H32"),
        8: ("Z12", "H10"),
        9: ("H11",),
        10: ("H12",),
    },
    after_gate={
        5: ("M01",),
        6: ("M02",),
        7: ("M03",),
        8: ("K00",),
    },
)
INNER_PLAN = dict(
    gates=("20", "00", "30", "--", "--", "--", "--"),
    downs=("--", "--", "--", "20", "00", "30", "10"),
    before_down={
        3: ("T20",),
        4: ("R20", "R21", "T00"),
        5: ("T30",),
        6: ("R22", "T10"),
    },
    before_gate={
        0: ("P00", "P01", "P02", "X00", "W00", "D00", "E00", "Q00", "S00", "Q01", "Q02", "L00"),
        2: ("B30", "B31", "B32"),
        3: ("M00", "K00", "M01", "M02", "M03"),
    },
    after_gate={
    },
)
AFTER_STEPS = ("30", "31", "00", "32")
BESIDE_MIXER = {0: ("R01",), 1: ("R02",)}

norm_floor = 0.5


def shifted(value, axis, steps):
    count = lax.axis_size(axis)
    leading, last = (max(0, -steps), min(count, count - steps))
    return lax.ppermute(value, axis, [(source, source + steps) for source in range(leading, last)])


def layer_norm(tokens, norm_gain):
    widened = tokens.astype(jnp.float32)
    centred = widened - jnp.mean(widened, axis=-1, keepdims=True)
    spread = jnp.mean(centred * centred, axis=-1, keepdims=True)
    return (centred * lax.rsqrt(spread + norm_floor) * norm_gain).astype(jnp.bfloat16)


def expert_hidden(inputs, gate_part, up_part):
    gate_value = jnp.dot(inputs, gate_part, preferred_element_type=jnp.float32)
    up_value = jnp.dot(inputs, up_part, preferred_element_type=jnp.float32)
    return (jax.nn.silu(gate_value) * up_value).astype(jnp.bfloat16)


def slot_ranks(route_ids, experts, lanes):
    tok_count, top_count = route_ids.shape
    grouped = route_ids.reshape(lanes, tok_count // lanes * top_count)
    onehot = (grouped[:, :, None] == jnp.arange(experts, dtype=jnp.int32)[None, None, :]).astype(
        jnp.int32
    )
    before = jnp.cumsum(onehot, axis=1) - onehot
    return jnp.sum(before * onehot, axis=2).reshape(tok_count, top_count)


def plain(
    out_gate,
    in_gate,
    values,
    conv_taps,
    mixer_weight,
    expert_input,
    norm_gain,
    route_ids,
    route_weights,
    gate_weight,
    up_weight,
    down_weight,
    shared_gate,
    shared_up,
    shared_down,
):
    experts = lax.axis_size("ep")
    lanes = lax.axis_size("tp")
    lane_rows = expert_input.shape[0]
    width = expert_input.shape[1]
    tok_count, top_count = route_ids.shape
    capacity = (2 * lane_rows * top_count + experts - 1) // experts
    gated_values = (in_gate.astype(jnp.float32) * values.astype(jnp.float32)).astype(jnp.bfloat16)
    previous = shifted(gated_values[-2:], "ep", 1)
    extended = jnp.concatenate([previous, gated_values], axis=0).astype(jnp.float32)
    conv_state = (
        conv_taps[0] * extended[:-2] + conv_taps[1] * extended[1:-1] + conv_taps[2] * extended[2:]
    )
    mixed_rows = (out_gate.astype(jnp.float32) * conv_state).astype(jnp.bfloat16)
    normed_own = layer_norm(expert_input, norm_gain)
    mixed_whole, normed_rows = (
        lax.all_gather(mixed_rows, "tp", axis=1, tiled=True),
        lax.all_gather(normed_own, "tp", axis=0, tiled=True),
    )
    mixer_output = jnp.dot(mixed_whole, mixer_weight, preferred_element_type=jnp.float32).astype(
        jnp.bfloat16
    )
    shared_part = expert_hidden(normed_rows, shared_gate, shared_up)
    slot_index = slot_ranks(route_ids, experts, lanes)
    lane_of_row = (jnp.arange(tok_count, dtype=jnp.int32) // lane_rows)[:, None]
    positions = (route_ids * lanes + lane_of_row) * capacity + slot_index
    lane_index = lax.axis_index("tp")
    lane_ids = lax.dynamic_slice_in_dim(route_ids, lane_index * lane_rows, lane_rows, 0)
    lane_slots = lax.dynamic_slice_in_dim(slot_index, lane_index * lane_rows, lane_rows, 0)
    lane_places = lane_ids * capacity + lane_slots
    local_rows = jnp.broadcast_to(jnp.arange(lane_rows, dtype=jnp.int32)[:, None], lane_ids.shape)
    owners = jnp.full((experts * capacity,), lane_rows, jnp.int32)
    owners = owners.at[lane_places.reshape(-1)].set(local_rows.reshape(-1))
    outgoing = jnp.take(normed_own, owners, axis=0, mode="fill", fill_value=0)
    arrived = lax.all_to_all(
        outgoing.reshape(experts, capacity, width), "ep", split_axis=0, concat_axis=0, tiled=True
    )
    segment = lax.all_gather(arrived[None], "tp", axis=0, tiled=True)
    hidden_rows = expert_hidden(segment.reshape(-1, width), gate_weight[0], up_weight[0])
    spread_hidden = hidden_rows.reshape(segment.shape[:-1] + (hidden_rows.shape[-1],))
    routed_hidden = jnp.swapaxes(spread_hidden, 0, 1).reshape(-1, spread_hidden.shape[-1])
    routed_whole, shared_whole = (
        lax.all_gather(routed_hidden, "tp", axis=1, tiled=True),
        lax.all_gather(shared_part, "tp", axis=1, tiled=True),
    )
    routed_result = jnp.dot(
        routed_whole, down_weight[0], preferred_element_type=jnp.float32
    ).astype(jnp.bfloat16)
    out_cols = routed_result.shape[-1]
    returned = lax.all_to_all(
        routed_result.reshape(experts, lanes * capacity, out_cols),
        "ep",
        split_axis=0,
        concat_axis=0,
        tiled=True,
    )
    shared_result = jnp.dot(shared_whole, shared_down, preferred_element_type=jnp.float32)
    picked = jnp.take(
        returned.reshape(experts * lanes * capacity, out_cols), positions.reshape(-1), axis=0
    )
    picked = picked.astype(jnp.float32).reshape(tok_count, top_count, out_cols)
    expert_output = (shared_result + jnp.sum(route_weights[:, :, None] * picked, axis=1)).astype(
        jnp.bfloat16
    )
    return (mixer_output, expert_output)


def silu_product(gate_value, up_value):
    return (gate_value * (1.0 / (1.0 + jnp.exp(-gate_value))) * up_value).astype(jnp.bfloat16)


def dot32(left, right):
    return jnp.dot(left, right, preferred_element_type=jnp.float32)


def kernel(
    n_ep,
    n_tp,
    ids_h,
    rw_h,
    og_h,
    ig_h,
    va_h,
    taps_h,
    mw_h,
    ei_h,
    ng_h,
    gw_h,
    uw_h,
    dw_h,
    sg_h,
    su_h,
    sd_h,
    mix_out,
    exp_out,
    og,
    ig,
    va,
    taps,
    mw,
    ei,
    ng,
    gw,
    uw,
    dw,
    sg,
    su,
    sd,
    ids,
    rw,
    tok,
    hid,
    shd,
    mixed,
    gated,
    halo,
    res,
    pin,
    acc,
    wcol,
    wts,
    ld,
    z_send,
    z_recv,
    x_send,
    x_recv,
    p_send,
    p_recv,
    r_send,
    r_recv,
    w_send,
    w_recv,
    h_sem,
):
    e = lax.axis_index("ep")
    t = lax.axis_index("tp")
    n_x = n_tp // CORES
    partner = t + 1 - 2 * (t % CORES)
    lane_rows, width = ei.shape
    rows, chans = og.shape

    pieces = lane_rows // PIECE
    loads = {}

    def load(name, src, dst):
        loads[name] = pltpu.make_async_copy(src, dst, ld.at[len(loads)])
        loads[name].start()

    for q in range(pieces):
        load(f"ei{q}", ei_h.at[pl.ds(q * PIECE, PIECE)], ei.at[pl.ds(q * PIECE, PIECE)])
    load("ng", ng_h, ng)

    barrier = pltpu.get_barrier_semaphore()
    greeted = [{"ep": (e + d) % n_ep, "tp": t} for d in range(1, n_ep)]
    greeted += [{"ep": e, "tp": (t + CORES * d) % n_tp} for d in range(1, n_x)]
    greeted += [{"ep": e, "tp": partner}]
    for peer in greeted:
        pl.semaphore_signal(barrier, inc=1, device_id=peer, device_id_type=MESH)

    for name, src, dst in (
        ("ids", ids_h, ids),
        ("rw", rw_h, rw),
        ("ig", ig_h, ig),
        ("va", va_h, va),
    ):
        load(name, src, dst)

    def remote(src, dst, send, recv, ep, tp):
        return pltpu.make_async_remote_copy(
            src_ref=src,
            dst_ref=dst,
            send_sem=send,
            recv_sem=recv,
            device_id={"ep": ep, "tp": tp},
            device_id_type=MESH,
        )

    def cross(slot, g, d, lane):
        return remote(
            slot(lane), slot(lane), x_send.at[slot.kind], x_recv.at[g, d - 1],
            e, (t + CORES * d) % n_tp,
        )

    def across(slot, g, d, lane):
        return remote(slot(lane), slot(lane), p_send.at[slot.kind], p_recv.at[g, d], e, partner)

    def from_x(d):
        return (t + n_tp - CORES * d) % n_tp

    def from_partner(d):
        return (partner + n_tp - CORES * d) % n_tp

    def gather_start(slot, g):
        for d in range(1, n_x):
            cross(slot, g, d, t).start()
        across(slot, g, 0, t).start()

    def gather_forward(slot, g):
        for d in range(1, n_x):
            cross(slot, g, d, from_x(d)).wait_recv()
            across(slot, g, d, from_x(d)).start()

    def gather_finish(slot, g):
        for d in range(n_x):
            across(slot, g, d, from_partner(d)).wait_recv()

    first_hidden = n_ep * pieces
    shared_g = 2 * first_hidden
    mixed_g = shared_g + 1
    strip = rows // CHUNKS

    class Slot:
        def __init__(self, kind, at):
            self.kind, self.at = kind, at

        def __call__(self, lane):
            return self.at(lane)

    def tok_slot(j, q):
        return Slot(0, lambda lane: tok.at[j, lane, q])

    def hid_slot(j, q):
        return Slot(1, lambda lane: hid.at[j, q, lane])

    def hid_g(j, q):
        return first_hidden + j * pieces + q

    shd_slot = Slot(2, lambda lane: shd.at[lane])

    def mixed_slot(k):
        return Slot(3, lambda lane: mixed.at[lane, pl.ds(k * strip, strip)])

    last = n_ep - 1
    flipped = e > last - e
    inner = (e > 0) & (e < last)
    up = jnp.where(flipped, e - 1, e + 1)
    down = jnp.clip(jnp.where(flipped, e + 1, e - 1), 0, last)

    def block_at(m):
        return jnp.where(flipped, last - m, m)

    def z_copy(side, d, j, q, own=0):
        block = tok.at[j, from_x(d), q]
        return remote(block, block, z_send.at[side + own * side], z_recv.at[d, j, q],
                      up if side == 0 else down, t)

    def arrive(m, q, onward=None, crosses=True):
        j = block_at(m)
        z_copy(0, 0, j, q).wait_recv()
        if onward is not None:
            z_copy(onward, 0, j, q).start()
        if crosses:
            for d in range(1, n_x):
                cross(tok_slot(j, q), j * pieces + q, d, t).start()
        across(tok_slot(j, q), j * pieces + q, 0, t).start()

    def arrive_beside(m, q):
        j = block_at(m)
        for d in range(1, n_x):
            z_copy(0, d, j, q).wait_recv()
            across(tok_slot(j, q), j * pieces + q, d, from_x(d)).start()

    def crossed(m, q, onward=None):
        j = block_at(m)
        for d in range(1, n_x):
            cross(tok_slot(j, q), j * pieces + q, d, from_x(d)).wait_recv()
            if onward is not None:
                z_copy(onward, d, j, q).start()
            across(tok_slot(j, q), j * pieces + q, d, from_x(d)).start()

    def own_onward(side, d, q):
        z_copy(side, d, e, q, own=1).start()

    part_rows = n_tp * PIECE
    halves = part_rows // SUB

    def half(h):
        return pl.ds(h * halves, halves)

    def hop(j, q, h):
        after = jnp.clip(jnp.where(j > e, e + 1, e - 1), 0, last)
        slot = jnp.where((j < e) & (after == j), n_ep, j)
        return remote(res.at[j, q, half(h)], pin.at[slot, q, half(h)],
                      r_send.at[0], r_recv.at[slot, q, h], after, t)

    def hop_arrives(slot, q, h):
        remote(res.at[0, q, half(h)], pin.at[slot, q, half(h)], r_send.at[0],
               r_recv.at[slot, q, h], jnp.clip(e + 1, 0, last), t).wait_recv()

    def relay(m, q):
        j = block_at(m)
        with jax.named_scope(f"relay{m}{q}"):
            for h in range(SUB):
                hop_arrives(j, q, h)
                total = res[j, q, half(h)].astype(jnp.float32) + pin[j, q, half(h)].astype(jnp.float32)
                res[j, q, half(h)] = total.astype(jnp.bfloat16)
                hop(j, q, h).start()

    def weights_to(d):
        return remote(wts.at[e], wts.at[e], w_send.at[0], w_recv.at[e], (e + d) % n_ep, t)

    def weight_column(j):
        held = wts[j]
        mine = jnp.where(lax.broadcasted_iota(jnp.int32, held.shape, 0) == e, held, 0.0)
        line = jnp.sum(mine, axis=0, keepdims=True)
        shape = (rows, held.shape[1])
        same = lax.broadcasted_iota(jnp.int32, shape, 0) == lax.broadcasted_iota(jnp.int32, shape, 1)
        return jnp.sum(jnp.where(same, line, 0.0), axis=1, keepdims=True)

    loads["ng"].wait()
    for q in range(pieces):
        loads[f"ei{q}"].wait()
        widened = ei[q * PIECE : (q + 1) * PIECE, :].astype(jnp.float32)
        centred = widened - jnp.mean(widened, axis=-1, keepdims=True)
        spread_of = jnp.mean(centred * centred, axis=-1, keepdims=True)
        normed = centred * lax.rsqrt(spread_of + norm_floor) * ng[...]
        tok[e, t, q] = normed.astype(jnp.bfloat16)

    for name, src, dst in (
        ("gw", gw_h, gw),
        ("uw", uw_h, uw),
        ("og", og_h, og),
        ("taps", taps_h, taps),
        ("sg", sg_h, sg),
        ("su", su_h, su),
        ("dw", dw_h, dw),
        ("sd", sd_h, sd),
        ("mw", mw_h, mw),
    ):
        load(name, src, dst)

    with jax.named_scope("barrier"):
        pl.semaphore_wait(barrier, len(greeted))

    for q in range(pieces):
        own_onward(0, 0, q)

        if q < pieces - 1:

            @pl.when(inner)
            def _():
                own_onward(1, 0, q)

        for d in range(1, n_x):
            cross(tok_slot(e, q), e * pieces + q, d, t).start()
        across(tok_slot(e, q), e * pieces + q, 0, t).start()

    loads["ids"].wait()
    loads["rw"].wait()
    place = lax.broadcasted_iota(jnp.int32, (wts.shape[1], rows), 0)
    dense = jnp.zeros(place.shape, jnp.float32)
    for k in range(ids.shape[0]):
        dense += jnp.where(ids[k : k + 1, :] == place, rw[k : k + 1, :], 0.0)
    wts[e] = jnp.zeros(wts.shape[1:], jnp.float32)
    wts[e, :, 0:rows] = dense
    for d in range(1, n_ep):
        weights_to(d).start()

    loads["ig"].wait()
    loads["va"].wait()

    def gate_cols(c, _):
        at = pl.ds(pl.multiple_of(c * 128, 128), 128)
        gated[:, at] = (ig[:, at].astype(jnp.float32) * va[:, at].astype(jnp.float32)).astype(
            jnp.bfloat16
        )
        return 0

    lax.fori_loop(0, chans // 128, gate_cols, 0)

    def halo_copy():
        return remote(gated.at[pl.ds(rows - 16, 16)], halo, h_sem.at[0], h_sem.at[1],
                      jnp.minimum(e + 1, last), t)

    @pl.when(e < last)
    def _():
        halo_copy().start()

    @pl.when(e == 0)
    def _():
        halo[...] = jnp.zeros_like(halo)

    for here, slot in ((e > 0, e), (e < last, n_ep)):

        @pl.when(~here)
        def _():
            pin[slot] = jnp.zeros(pin.shape[1:], pin.dtype)

    def mix_cols(c, _):
        at = pl.ds(pl.multiple_of(c * 128, 128), 128)
        now = gated[:, at].astype(jnp.float32)
        before = halo[:, at].astype(jnp.float32)
        place = lax.broadcasted_iota(jnp.int32, now.shape, 0)
        one = jnp.where(place == 0, before[15:16], pltpu.roll(now, 1, 0))
        two = jnp.where(
            place == 0, before[14:15], jnp.where(place == 1, before[15:16], pltpu.roll(now, 2, 0))
        )
        state = taps[0:1, at] * two + taps[1:2, at] * one + taps[2:3, at] * now
        mixed[t, :, at] = (og[:, at].astype(jnp.float32) * state).astype(jnp.bfloat16)
        return 0

    def mix():
        with jax.named_scope("mix"):
            loads["og"].wait()
            loads["taps"].wait()

            @pl.when(e > 0)
            def _():
                halo_copy().wait_recv()

            lax.fori_loop(0, chans // 128, mix_cols, 0)

    def weigh():
        def column(j, _):
            @pl.when(j != e)
            def _():
                remote(wts.at[e], wts.at[j], w_send.at[0], w_recv.at[j], j, t).wait_recv()

            spread_out = jnp.broadcast_to(weight_column(j), (rows, wcol.shape[-1]))
            spread_out = spread_out.reshape(n_tp, pieces, PIECE, wcol.shape[-1])
            for q in range(pieces):
                wcol[j, q] = spread_out[:, q].reshape(part_rows, wcol.shape[-1])
            return 0

        with jax.named_scope("weigh"):
            lax.fori_loop(0, n_ep, column, 0)

    def own_late():
        own_onward(1, 0, pieces - 1)
        for d in range(1, n_x):
            for q in range(pieces):
                own_onward(1, d, q)

    def own_crossed(q):
        crossed(0, q, onward=0)

    def inner_pair(q):
        arrive(0, q, onward=0, crosses=False)
        arrive(2, q, onward=1)
        crossed(1, q)

    def inner_far(q):
        arrive(3, q, onward=1)
        arrive_beside(0, q)
        crossed(2, q)

    def passed(m, q):
        j = block_at(m)
        gather_forward(hid_slot(j, q), hid_g(j, q))

    def mixed_out(k):
        gather_start(mixed_slot(k), mixed_g + k)

    def share():
        with jax.named_scope("shared"):
            block = tok[e].reshape(rows, width)
            shd[t] = silu_product(dot32(block, sg[...]), dot32(block, su[...]))

    def landed():
        for name in ("gw", "uw", "sg", "su", "dw"):
            loads[name].wait()

    acts = {
        "A": lambda m, q: arrive(m, q),
        "N": lambda m, q: arrive(m, q, crosses=False),
        "B": lambda m, q: crossed(m, q),
        "O": lambda m, q: own_crossed(q),
        "Z": lambda m, q: arrive_beside(m, q),
        "P": lambda m, q: inner_pair(q),
        "Q": lambda m, q: inner_far(q),
        "L": lambda m, q: own_late(),
        "H": lambda m, q: passed(m, q),
        "T": lambda m, q: [passed(m, each) for each in range(pieces)],
        "R": lambda m, q: relay(m, q),
        "M": lambda m, q: mixed_out(q),
        "X": lambda m, q: mix(),
        "W": lambda m, q: weigh(),
        "S": lambda m, q: share(),
        "D": lambda m, q: landed(),
        "E": lambda m, q: gate_block(e, 0, send=False),
        "K": lambda m, q: own_out(),
    }

    def table(names, r, k, unroll):
        found = jnp.int32(-1)
        for at, name in enumerate(names):
            if at % unroll == k and name != "--":
                found = jnp.where(r == at // unroll, int(name[0]) * pieces + int(name[1]), found)
        return found

    def due(part, r, k=0, unroll=1):
        for at, what in part.items():
            if at % unroll == k:

                @pl.when(r == at // unroll)
                def _():
                    for one in what:
                        acts[one[0]](int(one[1]), int(one[2]))

    def down_tiles(weight, hidden, place):
        part = hid.shape[-1]
        for c in range(chans // TILE):
            at = slice(c * TILE, (c + 1) * TILE)
            total = dot32(hidden(0), dw[0:part, at])
            for lane in range(1, n_tp):
                total += dot32(hidden(lane), dw[lane * part : (lane + 1) * part, at])
            place(at, (weight * total).astype(jnp.bfloat16))

    def down_piece(j, q):
        with jax.named_scope("hid_wait"):
            gather_finish(hid_slot(j, q), hid_g(j, q))

        def place(at, found):
            res[j, q, :, at] = found

        with jax.named_scope("down"):
            down_tiles(wcol[j, q][:, 0:1], lambda lane: hid[j, q, lane], place)
        for h in range(SUB):
            hop(j, q, h).start()

    def down_block(j, q):
        with jax.named_scope("hid_wait"):
            for q in range(pieces):
                gather_finish(hid_slot(j, q), hid_g(j, q))

        def place(at, found):
            res[j, :, :, at] = found.reshape(pieces, part_rows, TILE)

        with jax.named_scope("down"):
            down_tiles(
                wcol[j].reshape(rows, wcol.shape[-1])[:, 0:1],
                lambda lane: hid[j, :, lane].reshape(rows, hid.shape[-1]),
                place,
            )

    def gate_block(j, q, send=True):
        with jax.named_scope("gate_wait"):
            for q in range(pieces):
                gather_finish(tok_slot(j, q), j * pieces + q)

        with jax.named_scope("gate"):
            block = tok[j].reshape(rows, width)
            made = silu_product(dot32(block, gw[...]), dot32(block, uw[...]))
            made = made.reshape(n_tp, pieces, PIECE, made.shape[-1])
            for q in range(pieces):
                hid[j, q, t] = made[:, q].reshape(part_rows, made.shape[-1])
                if send:
                    gather_start(hid_slot(j, q), hid_g(j, q))

    def own_out():
        for q in range(pieces):
            gather_start(hid_slot(e, q), hid_g(e, q))
        gather_start(shd_slot, shared_g)

    def gate_piece(j, q):
        with jax.named_scope("gate_wait"):
            gather_finish(tok_slot(j, q), j * pieces + q)

        with jax.named_scope("gate"):
            block = tok[j, :, q].reshape(part_rows, width)
            hid[j, q, t] = silu_product(dot32(block, gw[...]), dot32(block, uw[...]))
            gather_start(hid_slot(j, q), hid_g(j, q))

    def run(plan, unroll, gate, down):
        def step(r, _):
            for k in range(unroll):
                with jax.named_scope("pre_down"):
                    due(plan["before_down"], r, k, unroll)
                if any(name != "--" for name in plan["downs"][k::unroll]):
                    down_at = table(plan["downs"], r, k, unroll)

                    @pl.when(down_at >= 0)
                    def _():
                        down(block_at(down_at // pieces), down_at % pieces)

                with jax.named_scope("pre_gate"):
                    due(plan["before_gate"], r, k, unroll)
                gate_at = table(plan["gates"], r, k, unroll)

                @pl.when(gate_at >= 0)
                def _():
                    gate(block_at(gate_at // pieces), gate_at % pieces)

                due(plan["after_gate"], r, k, unroll)

            return 0

        lax.fori_loop(0, -(-len(plan["gates"]) // unroll), step, 0)

    @pl.when(~inner)
    def _():
        run(END_PLAN, STEPS, gate_piece, down_piece)

    @pl.when(inner)
    def _():
        run(INNER_PLAN, 1, gate_block, down_block)

    @pl.when(~inner)
    def _():
        for q in range(pieces):
            passed(0, q)
        down_block(e, 0)

    @pl.when(inner)
    def _():
        for one in AFTER_STEPS:
            relay(int(one[0]), int(one[1]))

    with jax.named_scope("acc"):
        gather_forward(shd_slot, shared_g)
        loads["sd"].wait()
        gather_finish(shd_slot, shared_g)

        def shared_cols(c, _):
            at = pl.ds(pl.multiple_of(c * TILE, TILE), TILE)
            part = shd.shape[-1]
            total = dot32(shd[0], sd[0:part, at])
            for lane in range(1, n_tp):
                total += dot32(shd[lane], sd[lane * part : (lane + 1) * part, at])
            acc[:, :, :, at] = total.reshape(n_tp, pieces, PIECE, TILE)
            return 0

        lax.fori_loop(0, chans // TILE, shared_cols, 0)

    with jax.named_scope("mixed_wait"):
        loads["mw"].wait()
        for k in range(CHUNKS):
            gather_forward(mixed_slot(k), mixed_g + k)
        for k in range(CHUNKS):
            gather_finish(mixed_slot(k), mixed_g + k)

    def mixer_cols(c, _):
        with jax.named_scope("mixer"):
            at = pl.ds(pl.multiple_of(c * TILE, TILE), TILE)
            total = dot32(mixed[0], mw[0:chans, at])
            for lane in range(1, n_tp):
                total += dot32(mixed[lane], mw[lane * chans : (lane + 1) * chans, at])
            mix_out[:, at] = total.astype(jnp.bfloat16)


        @pl.when(inner)
        def _():
            due(BESIDE_MIXER, c)

        return 0

    lax.fori_loop(0, chans // TILE, mixer_cols, 0)

    def combine(q, _):
        with jax.named_scope("final_wait"):
            for here, slot in ((e > 0, e), (e < last, n_ep)):

                @pl.when(here)
                def _():
                    for h in range(SUB):
                        hop_arrives(slot, q, h)

        total = acc[:, q].reshape(part_rows, chans)
        for found in (res[e, q], pin[e, q], pin[n_ep, q]):
            total += found.astype(jnp.float32)
        whole = total.astype(jnp.bfloat16)
        for lane in range(n_tp):
            at = pl.ds(pl.multiple_of(lane * lane_rows + q * PIECE, PIECE), PIECE)
            exp_out[at, :] = whole[lane * PIECE : (lane + 1) * PIECE]
        return 0

    lax.fori_loop(0, pieces, combine, 0)

    @pl.when(e < last)
    def _():
        halo_copy().wait_send()

    def sent(ref, sem):
        remote(ref, ref, sem, h_sem.at[1], e, partner).wait_send()

    with jax.named_scope("drain"):

        @pl.when(~inner)
        def _():
            sent(tok.at[0, 0:n_x], z_send.at[0])

        @pl.when(inner)
        def _():
            sent(tok.at[0:2, 0], z_send.at[0])
            sent(tok.at[0 : n_ep - 2, 0], z_send.at[1])
            sent(tok.at[0, 0:n_x], z_send.at[2])

        sent(tok.at[0 : n_ep - 1, 0 : n_x - 1], x_send.at[0])
        sent(tok.at[:, 0:n_x], p_send.at[0])
        sent(hid.at[:, :, 0 : n_x - 1], x_send.at[1])
        sent(hid.at[:, :, 0:n_x], p_send.at[1])
        sent(shd.at[0 : n_x - 1], x_send.at[2])
        sent(shd.at[0:n_x], p_send.at[2])
        sent(mixed.at[0 : n_x - 1], x_send.at[3])
        sent(mixed.at[0:n_x], p_send.at[3])
        sent(res.at[0 : n_ep - 1], r_send.at[0])
        sent(wts.at[0 : n_ep - 1], w_send.at[0])


def joined(n_ep, n_tp, *args):
    (og, ig, va, taps, mw, ei, ng, ids, rw, gw, uw, dw, sg, su, sd) = args
    gw, uw, dw, ng = gw[0], uw[0], dw[0], ng[None]
    bf, f32 = jnp.bfloat16, jnp.float32
    rows, chans = og.shape
    lane_rows, width = ei.shape
    n_x = n_tp // CORES
    pieces = lane_rows // PIECE
    sems = 2 * n_ep * pieces + 1 + CHUNKS
    big = (og, ig, va, taps, mw, ei, ng, gw, uw, dw, sg, su, sd)
    out = pltpu.VMEM((rows, chans), bf)
    vmem = pl.BlockSpec(memory_space=pltpu.VMEM)
    dma = pltpu.SemaphoreType.DMA
    return pl.pallas_call(
        functools.partial(kernel, n_ep, n_tp),
        out_shape=(out, out),
        in_specs=[pl.BlockSpec(memory_space=pl.ANY)] * (2 + len(big)),
        out_specs=(vmem, vmem),
        scratch_shapes=[pltpu.VMEM(a.shape, a.dtype) for a in (*big, ids.T, rw.T)]
        + [
            pltpu.VMEM((n_ep, n_tp, pieces, PIECE, width), bf),
            pltpu.VMEM((n_ep, pieces, n_tp, n_tp * PIECE, gw.shape[-1]), bf),
            pltpu.VMEM((n_tp, rows, sg.shape[-1]), bf),
            pltpu.VMEM((n_tp, rows, chans), bf),
            pltpu.VMEM((rows, chans), bf),
            pltpu.VMEM((16, chans), bf),
            pltpu.VMEM((n_ep, pieces, n_tp * PIECE, chans), bf),
            pltpu.VMEM((n_ep + 1, pieces, n_tp * PIECE, chans), bf),
            pltpu.VMEM((n_tp, pieces, PIECE, chans), f32),
            pltpu.VMEM((n_ep, pieces, n_tp * PIECE, 128), f32),
            pltpu.VMEM((n_ep, -(-n_ep // 8) * 8, -(-rows // 128) * 128), f32),
            dma((len(big) + 1 + pieces,)),
            dma((3,)),
            dma((n_x, n_ep, pieces)),
            dma((4,)),
            dma((sems, max(1, n_x - 1))),
            dma((4,)),
            dma((sems, n_x)),
            dma((1,)),
            dma((n_ep + 1, pieces, SUB)),
            dma((1,)),
            dma((n_ep,)),
            dma((2,)),
        ],
        compiler_params=pltpu.CompilerParams(
            collective_id=0, has_side_effects=True, vmem_limit_bytes=60 * 1024 * 1024
        ),
    )(ids.T, rw.T, *big)


def local(*args):
    n_ep, n_tp = lax.axis_size("ep"), lax.axis_size("tp")
    chans, lane_rows = args[0].shape[1], args[5].shape[0]
    aligned = (
        n_tp % CORES == 0
        and n_ep == 2 * ROLES
        and lane_rows == STEPS * PIECE
        and lane_rows % PIECE == 0
        and lane_rows * n_tp == args[0].shape[0]
        and chans % TILE == 0
        and args[0].shape[0] % (16 * CHUNKS) == 0
        and args[9].shape[2] % 128 == 0
        and args[12].shape[1] % 128 == 0
    )
    return joined(n_ep, n_tp, *args) if aligned else plain(*args)


def solution(mesh):
    placed = (
        P(("grp", "ep"), "tp"),
        P(("grp", "ep"), "tp"),
        P(("grp", "ep"), "tp"),
        P(None, "tp"),
        P(None, "tp"),
        P(("grp", "ep", "tp"), None),
        P(),
        P(("grp", "ep"), None),
        P(("grp", "ep"), None),
        P("ep", None, "tp"),
        P("ep", None, "tp"),
        P("ep", None, "tp"),
        P(None, "tp"),
        P(None, "tp"),
        P(None, "tp"),
    )
    return jax.shard_map(
        local,
        mesh=mesh,
        in_specs=placed,
        out_specs=(P(("grp", "ep"), "tp"), P(("grp", "ep"), "tp")),
        check_vma=False,
    )
```

```python
import functools

import jax
import jax.numpy as jnp
from jax import lax
from jax.experimental import pallas as pl
from jax.experimental.pallas import tpu as pltpu
from jax.sharding import PartitionSpec as P

MESH = pl.DeviceIdType.MESH
CORES = 2
TILE = 256
PIECE = 16
CHUNKS = 4
ROLES = 2
MIX_TILES = 4
STEPS = 3
SUB = 2

END_PLAN = dict(
    gates=("20", "30", "21", "31", "--", "12", "32", "--", "22", "10", "11", "--", "--"),
    downs=("--", "--", "--", "20", "30", "21", "--", "31", "32", "12", "22", "10", "11"),
    before_down={
        0: ("c02", "c01", "u01", "u02", "A20", "A21", "O01", "D00", "O00", "O02", "N10", "B20", "A30", "E00"),
        1: ("k01", "S00", "X00", "A31", "B30", "k02", "B21"),
        3: ("H20", "A32", "B31", "W00"),
        7: ("H31", "k00", "B22", "M03"),
        10: ("H00", "M00", "N11", "M01", "H22", "Z11", "V03", "Y00"),
    },
    before_gate={
        3: ("s00", "H30", "H21", "Z12"),
        4: ("N12",),
        5: ("A22", "B32"),
        7: ("Z10", "M02", "H02", "U00", "H01", "H32", "H12"),
        10: ("H10", "V02"),
        11: ("V00", "C00", "H11", "V01"),
    },
    after_gate={},
)
INNER_PLAN = dict(
    gates=("00", "30", "20", "--", "--", "--"),
    downs=("--", "--", "30", "00", "20", "10"),
    before_down={
        0: ("c02", "u01", "c01", "a20", "a00", "a21", "b02", "a01", "a30", "a02", "a31", "b00", "u02", "a32", "B20", "l12", "X00", "B30", "Z01", "b01", "Z00", "D00", "Z02", "l02", "B31", "a22", "E00"),
        1: ("B32",),
        2: ("W00", "l10", "S00", "l01", "B21", "B22", "H31", "H00", "k00", "l11", "k01", "M03", "H32", "H30"),
    },
    before_gate={
        2: ("R30", "H02", "H01"),
        3: ("M00", "H10", "R31", "H20", "s00", "R00", "H22", "H11", "H21", "k02", "R32", "M02"),
        4: ("R20", "M01", "V00", "H12", "R01", "R21", "V03", "U00"),
    },
    after_gate={},
)
END_AFTER = ("m00", "m01", "m02", "m03")
INNER_AFTER = ("R02", "V01", "V02", "R22", "C00", "m00", "m01", "m02", "m03")

norm_floor = 0.5


def shifted(value, axis, steps):
    count = lax.axis_size(axis)
    leading, last = (max(0, -steps), min(count, count - steps))
    return lax.ppermute(value, axis, [(source, source + steps) for source in range(leading, last)])


def layer_norm(tokens, norm_gain):
    widened = tokens.astype(jnp.float32)
    centred = widened - jnp.mean(widened, axis=-1, keepdims=True)
    spread = jnp.mean(centred * centred, axis=-1, keepdims=True)
    return (centred * lax.rsqrt(spread + norm_floor) * norm_gain).astype(jnp.bfloat16)


def expert_hidden(inputs, gate_part, up_part):
    gate_value = jnp.dot(inputs, gate_part, preferred_element_type=jnp.float32)
    up_value = jnp.dot(inputs, up_part, preferred_element_type=jnp.float32)
    return (jax.nn.silu(gate_value) * up_value).astype(jnp.bfloat16)


def slot_ranks(route_ids, experts, lanes):
    tok_count, top_count = route_ids.shape
    grouped = route_ids.reshape(lanes, tok_count // lanes * top_count)
    onehot = (grouped[:, :, None] == jnp.arange(experts, dtype=jnp.int32)[None, None, :]).astype(
        jnp.int32
    )
    before = jnp.cumsum(onehot, axis=1) - onehot
    return jnp.sum(before * onehot, axis=2).reshape(tok_count, top_count)


def plain(
    out_gate,
    in_gate,
    values,
    conv_taps,
    mixer_weight,
    expert_input,
    norm_gain,
    route_ids,
    route_weights,
    gate_weight,
    up_weight,
    down_weight,
    shared_gate,
    shared_up,
    shared_down,
):
    experts = lax.axis_size("ep")
    lanes = lax.axis_size("tp")
    lane_rows = expert_input.shape[0]
    width = expert_input.shape[1]
    tok_count, top_count = route_ids.shape
    capacity = (2 * lane_rows * top_count + experts - 1) // experts
    gated_values = (in_gate.astype(jnp.float32) * values.astype(jnp.float32)).astype(jnp.bfloat16)
    previous = shifted(gated_values[-2:], "ep", 1)
    extended = jnp.concatenate([previous, gated_values], axis=0).astype(jnp.float32)
    conv_state = (
        conv_taps[0] * extended[:-2] + conv_taps[1] * extended[1:-1] + conv_taps[2] * extended[2:]
    )
    mixed_rows = (out_gate.astype(jnp.float32) * conv_state).astype(jnp.bfloat16)
    normed_own = layer_norm(expert_input, norm_gain)
    mixed_whole, normed_rows = (
        lax.all_gather(mixed_rows, "tp", axis=1, tiled=True),
        lax.all_gather(normed_own, "tp", axis=0, tiled=True),
    )
    mixer_output = jnp.dot(mixed_whole, mixer_weight, preferred_element_type=jnp.float32).astype(
        jnp.bfloat16
    )
    shared_part = expert_hidden(normed_rows, shared_gate, shared_up)
    slot_index = slot_ranks(route_ids, experts, lanes)
    lane_of_row = (jnp.arange(tok_count, dtype=jnp.int32) // lane_rows)[:, None]
    positions = (route_ids * lanes + lane_of_row) * capacity + slot_index
    lane_index = lax.axis_index("tp")
    lane_ids = lax.dynamic_slice_in_dim(route_ids, lane_index * lane_rows, lane_rows, 0)
    lane_slots = lax.dynamic_slice_in_dim(slot_index, lane_index * lane_rows, lane_rows, 0)
    lane_places = lane_ids * capacity + lane_slots
    local_rows = jnp.broadcast_to(jnp.arange(lane_rows, dtype=jnp.int32)[:, None], lane_ids.shape)
    owners = jnp.full((experts * capacity,), lane_rows, jnp.int32)
    owners = owners.at[lane_places.reshape(-1)].set(local_rows.reshape(-1))
    outgoing = jnp.take(normed_own, owners, axis=0, mode="fill", fill_value=0)
    arrived = lax.all_to_all(
        outgoing.reshape(experts, capacity, width), "ep", split_axis=0, concat_axis=0, tiled=True
    )
    segment = lax.all_gather(arrived[None], "tp", axis=0, tiled=True)
    hidden_rows = expert_hidden(segment.reshape(-1, width), gate_weight[0], up_weight[0])
    spread_hidden = hidden_rows.reshape(segment.shape[:-1] + (hidden_rows.shape[-1],))
    routed_hidden = jnp.swapaxes(spread_hidden, 0, 1).reshape(-1, spread_hidden.shape[-1])
    routed_whole, shared_whole = (
        lax.all_gather(routed_hidden, "tp", axis=1, tiled=True),
        lax.all_gather(shared_part, "tp", axis=1, tiled=True),
    )
    routed_result = jnp.dot(
        routed_whole, down_weight[0], preferred_element_type=jnp.float32
    ).astype(jnp.bfloat16)
    out_cols = routed_result.shape[-1]
    returned = lax.all_to_all(
        routed_result.reshape(experts, lanes * capacity, out_cols),
        "ep",
        split_axis=0,
        concat_axis=0,
        tiled=True,
    )
    shared_result = jnp.dot(shared_whole, shared_down, preferred_element_type=jnp.float32)
    picked = jnp.take(
        returned.reshape(experts * lanes * capacity, out_cols), positions.reshape(-1), axis=0
    )
    picked = picked.astype(jnp.float32).reshape(tok_count, top_count, out_cols)
    expert_output = (shared_result + jnp.sum(route_weights[:, :, None] * picked, axis=1)).astype(
        jnp.bfloat16
    )
    return (mixer_output, expert_output)


def silu_product(gate_value, up_value):
    return (gate_value * (1.0 / (1.0 + jnp.exp(-gate_value))) * up_value).astype(jnp.bfloat16)


def dot32(left, right):
    return jnp.dot(left, right, preferred_element_type=jnp.float32)


def kernel(
    n_ep,
    n_tp,
    ids_h,
    rw_h,
    og_h,
    ig_h,
    va_h,
    taps_h,
    mw_h,
    ei_h,
    ng_h,
    gw_h,
    uw_h,
    dw_h,
    sg_h,
    su_h,
    sd_h,
    mix_out,
    exp_out,
    og,
    ig,
    va,
    taps,
    mw,
    ei,
    ng,
    gw,
    uw,
    dw,
    sg,
    su,
    sd,
    ids,
    rw,
    tok,
    hid,
    shd,
    mixed,
    gated,
    halo,
    res,
    pin,
    acc,
    wcol,
    wts,
    ld,
    z_send,
    z_recv,
    x_send,
    x_recv,
    p_send,
    p_recv,
    r_send,
    r_recv,
    w_send,
    w_recv,
    h_sem,
):
    e = lax.axis_index("ep")
    t = lax.axis_index("tp")
    n_x = n_tp // CORES
    partner = t + 1 - 2 * (t % CORES)
    lane_rows, width = ei.shape
    rows, chans = og.shape

    pieces = lane_rows // PIECE
    loads = {}

    def load(name, src, dst):
        loads[name] = pltpu.make_async_copy(src, dst, ld.at[len(loads)])
        loads[name].start()

    for q in range(pieces):
        load(f"ei{q}", ei_h.at[pl.ds(q * PIECE, PIECE)], ei.at[pl.ds(q * PIECE, PIECE)])
    load("ng", ng_h, ng)

    barrier = pltpu.get_barrier_semaphore()
    greeted = [{"ep": (e + d) % n_ep, "tp": t} for d in range(1, n_ep)]
    greeted += [{"ep": e, "tp": (t + CORES * d) % n_tp} for d in range(1, n_x)]
    greeted += [{"ep": e, "tp": partner}]
    for peer in greeted:
        pl.semaphore_signal(barrier, inc=1, device_id=peer, device_id_type=MESH)

    for name, src, dst in (
        ("ids", ids_h, ids),
        ("rw", rw_h, rw),
        ("ig", ig_h, ig),
        ("va", va_h, va),
    ):
        load(name, src, dst)

    def remote(src, dst, send, recv, ep, tp):
        return pltpu.make_async_remote_copy(
            src_ref=src,
            dst_ref=dst,
            send_sem=send,
            recv_sem=recv,
            device_id={"ep": ep, "tp": tp},
            device_id_type=MESH,
        )

    def cross(slot, g, d, lane):
        return remote(
            slot(lane), slot(lane), x_send.at[slot.kind], x_recv.at[g, d - 1],
            e, (t + CORES * d) % n_tp,
        )

    def across(slot, g, d, lane):
        return remote(slot(lane), slot(lane), p_send.at[slot.kind], p_recv.at[g, d], e, partner)

    def from_x(d):
        return (t + n_tp - CORES * d) % n_tp

    def from_partner(d):
        return (partner + n_tp - CORES * d) % n_tp

    def gather_start(slot, g):
        for d in range(1, n_x):
            cross(slot, g, d, t).start()
        across(slot, g, 0, t).start()

    def gather_forward(slot, g):
        for d in range(1, n_x):
            cross(slot, g, d, from_x(d)).wait_recv()
            across(slot, g, d, from_x(d)).start()

    def gather_finish(slot, g):
        for d in range(n_x):
            across(slot, g, d, from_partner(d)).wait_recv()

    first_hidden = n_ep * pieces
    shared_g = 2 * first_hidden
    mixed_g = shared_g + 1
    strip = rows // CHUNKS

    class Slot:
        def __init__(self, kind, at):
            self.kind, self.at = kind, at

        def __call__(self, lane):
            return self.at(lane)

    def tok_slot(j, q):
        return Slot(0, lambda lane: tok.at[j, lane, q])

    def hid_slot(j, q):
        return Slot(1, lambda lane: hid.at[j, q, lane])

    def hid_g(j, q):
        return first_hidden + j * pieces + q

    shd_slot = Slot(2, lambda lane: shd.at[lane])

    def mixed_slot(k):
        return Slot(3, lambda lane: mixed.at[lane, pl.ds(k * strip, strip)])

    last = n_ep - 1
    flipped = e > last - e
    inner = (e > 0) & (e < last)
    up = jnp.where(flipped, e - 1, e + 1)
    down = jnp.clip(jnp.where(flipped, e + 1, e - 1), 0, last)

    def block_at(m):
        return jnp.where(flipped, last - m, m)

    def z_copy(side, d, j, q, own=0):
        block = tok.at[j, from_x(d), q]
        return remote(block, block, z_send.at[side + own * side], z_recv.at[d, j, q],
                      up if side == 0 else down, t)

    def arrive(m, q, onward=None, crosses=True):
        j = block_at(m)
        z_copy(0, 0, j, q).wait_recv()
        if onward is not None:
            z_copy(onward, 0, j, q).start()
        if crosses:
            for d in range(1, n_x):
                cross(tok_slot(j, q), j * pieces + q, d, t).start()
        across(tok_slot(j, q), j * pieces + q, 0, t).start()

    def arrive_beside(m, q):
        j = block_at(m)
        for d in range(1, n_x):
            z_copy(0, d, j, q).wait_recv()
            across(tok_slot(j, q), j * pieces + q, d, from_x(d)).start()

    def crossed(m, q, onward=None):
        j = block_at(m)
        for d in range(1, n_x):
            cross(tok_slot(j, q), j * pieces + q, d, from_x(d)).wait_recv()
            if onward is not None:
                z_copy(onward, d, j, q).start()
            across(tok_slot(j, q), j * pieces + q, d, from_x(d)).start()

    def own_onward(side, d, q):
        z_copy(side, d, e, q, own=1).start()

    def own_across(q):
        gather_start(tok_slot(e, q), e * pieces + q)

    part_rows = n_tp * PIECE
    halves = part_rows // SUB

    def half(h):
        return pl.ds(h * halves, halves)

    def hop(j, q, h):
        after = jnp.clip(jnp.where(j > e, e + 1, e - 1), 0, last)
        slot = jnp.where((j < e) & (after == j), n_ep, j)
        return remote(res.at[j, q, half(h)], pin.at[slot, q, half(h)],
                      r_send.at[0], r_recv.at[slot, q, h], after, t)

    def hop_arrives(slot, q, h):
        remote(res.at[0, q, half(h)], pin.at[slot, q, half(h)], r_send.at[0],
               r_recv.at[slot, q, h], jnp.clip(e + 1, 0, last), t).wait_recv()

    def relay(m, q):
        j = block_at(m)
        with jax.named_scope(f"relay{m}{q}"):
            for h in range(SUB):
                hop_arrives(j, q, h)
                total = res[j, q, half(h)].astype(jnp.float32) + pin[j, q, half(h)].astype(jnp.float32)
                res[j, q, half(h)] = total.astype(jnp.bfloat16)
                hop(j, q, h).start()

    def weights_to(d):
        return remote(wts.at[e], wts.at[e], w_send.at[0], w_recv.at[e], (e + d) % n_ep, t)

    def weight_column(j):
        held = wts[j]
        mine = jnp.where(lax.broadcasted_iota(jnp.int32, held.shape, 0) == e, held, 0.0)
        line = jnp.sum(mine, axis=0, keepdims=True)
        shape = (rows, held.shape[1])
        same = lax.broadcasted_iota(jnp.int32, shape, 0) == lax.broadcasted_iota(jnp.int32, shape, 1)
        return jnp.sum(jnp.where(same, line, 0.0), axis=1, keepdims=True)

    loads["ng"].wait()
    for q in range(pieces):
        loads[f"ei{q}"].wait()
        widened = ei[q * PIECE : (q + 1) * PIECE, :].astype(jnp.float32)
        centred = widened - jnp.mean(widened, axis=-1, keepdims=True)
        spread_of = jnp.mean(centred * centred, axis=-1, keepdims=True)
        normed = centred * lax.rsqrt(spread_of + norm_floor) * ng[...]
        tok[e, t, q] = normed.astype(jnp.bfloat16)
        if q == 0:
            with jax.named_scope("barrier"):
                pl.semaphore_wait(barrier, len(greeted))
            own_onward(0, 0, q)

            @pl.when(inner)
            def _():
                own_onward(1, 0, q)

            own_across(q)

    for name, src, dst in (
        ("gw", gw_h, gw),
        ("uw", uw_h, uw),
        ("og", og_h, og),
        ("taps", taps_h, taps),
        ("sg", sg_h, sg),
        ("su", su_h, su),
        ("dw", dw_h, dw),
        ("sd", sd_h, sd),
        ("mw", mw_h, mw),
    ):
        load(name, src, dst)

    loads["ids"].wait()
    loads["rw"].wait()
    place = lax.broadcasted_iota(jnp.int32, (wts.shape[1], rows), 0)
    dense = jnp.zeros(place.shape, jnp.float32)
    for k in range(ids.shape[0]):
        dense += jnp.where(ids[k : k + 1, :] == place, rw[k : k + 1, :], 0.0)
    wts[e] = jnp.zeros(wts.shape[1:], jnp.float32)
    wts[e, :, 0:rows] = dense
    for d in range(1, n_ep):
        weights_to(d).start()

    loads["ig"].wait()
    loads["va"].wait()

    def gate_cols(c, _):
        at = pl.ds(pl.multiple_of(c * 128, 128), 128)
        gated[:, at] = (ig[:, at].astype(jnp.float32) * va[:, at].astype(jnp.float32)).astype(
            jnp.bfloat16
        )
        return 0

    lax.fori_loop(0, chans // 128, gate_cols, 0)

    def halo_copy():
        return remote(gated.at[pl.ds(rows - 16, 16)], halo, h_sem.at[0], h_sem.at[1],
                      jnp.minimum(e + 1, last), t)

    @pl.when(e < last)
    def _():
        halo_copy().start()

    @pl.when(e == 0)
    def _():
        halo[...] = jnp.zeros_like(halo)

    for here, slot in ((e > 0, e), (e < last, n_ep)):

        @pl.when(~here)
        def _():
            pin[slot] = jnp.zeros(pin.shape[1:], pin.dtype)

    def mix_cols(c, _):
        at = pl.ds(pl.multiple_of(c * 128, 128), 128)
        now = gated[:, at].astype(jnp.float32)
        before = halo[:, at].astype(jnp.float32)
        place = lax.broadcasted_iota(jnp.int32, now.shape, 0)
        one = jnp.where(place == 0, before[15:16], pltpu.roll(now, 1, 0))
        two = jnp.where(
            place == 0, before[14:15], jnp.where(place == 1, before[15:16], pltpu.roll(now, 2, 0))
        )
        state = taps[0:1, at] * two + taps[1:2, at] * one + taps[2:3, at] * now
        mixed[t, :, at] = (og[:, at].astype(jnp.float32) * state).astype(jnp.bfloat16)
        return 0

    def mix():
        with jax.named_scope("mix"):
            loads["og"].wait()
            loads["taps"].wait()

            @pl.when(e > 0)
            def _():
                halo_copy().wait_recv()

            lax.fori_loop(0, chans // 128, mix_cols, 0)

    def weigh():
        def column(j, _):
            @pl.when(j != e)
            def _():
                remote(wts.at[e], wts.at[j], w_send.at[0], w_recv.at[j], j, t).wait_recv()

            spread_out = jnp.broadcast_to(weight_column(j), (rows, wcol.shape[-1]))
            spread_out = spread_out.reshape(n_tp, pieces, PIECE, wcol.shape[-1])
            for q in range(pieces):
                wcol[j, q] = spread_out[:, q].reshape(part_rows, wcol.shape[-1])
            return 0

        with jax.named_scope("weigh"):
            lax.fori_loop(0, n_ep, column, 0)

    def own_crossed(q):
        crossed(0, q, onward=0)

    def inner_arrive(m, q):
        arrive(m, q, onward=0 if m == 0 else 1, crosses=m != 0)

    def passed(m, q):
        j = block_at(m)
        gather_forward(hid_slot(j, q), hid_g(j, q))

    def mixed_out(k):
        gather_start(mixed_slot(k), mixed_g + k)

    def share():
        with jax.named_scope("shared"):
            block = tok[e].reshape(rows, width)
            shd[t] = silu_product(dot32(block, sg[...]), dot32(block, su[...]))

    def landed():
        for name in ("gw", "uw", "sg", "su", "dw"):
            loads[name].wait()

    def shared_down():
        with jax.named_scope("acc"):
            loads["sd"].wait()
            gather_finish(shd_slot, shared_g)

            def shared_cols(c, _):
                at = pl.ds(pl.multiple_of(c * TILE, TILE), TILE)
                part = shd.shape[-1]
                total = dot32(shd[0], sd[0:part, at])
                for lane in range(1, n_tp):
                    total += dot32(shd[lane], sd[lane * part : (lane + 1) * part, at])
                acc[:, :, :, at] = total.reshape(n_tp, pieces, PIECE, TILE)
                return 0

            lax.fori_loop(0, chans // TILE, shared_cols, 0)

    def mixer_tile(c):
        if c == 0:
            with jax.named_scope("mixed_wait"):
                loads["mw"].wait()
                for k in range(CHUNKS):
                    gather_finish(mixed_slot(k), mixed_g + k)

        with jax.named_scope("mixer"):
            at = pl.ds(c * TILE, TILE)
            total = dot32(mixed[0], mw[0:chans, at])
            for lane in range(1, n_tp):
                total += dot32(mixed[lane], mw[lane * chans : (lane + 1) * chans, at])
            mix_out[:, at] = total.astype(jnp.bfloat16)

    acts = {
        "A": lambda m, q: arrive(m, q),
        "N": lambda m, q: arrive(m, q, crosses=False),
        "a": lambda m, q: inner_arrive(m, q),
        "B": lambda m, q: crossed(m, q),
        "O": lambda m, q: own_crossed(q),
        "b": lambda m, q: crossed(1, q),
        "Z": lambda m, q: arrive_beside(m, q),
        "l": lambda m, q: own_onward(1, m, q),
        "H": lambda m, q: passed(m, q),
        "R": lambda m, q: relay(m, q),
        "M": lambda m, q: mixed_out(q),
        "V": lambda m, q: gather_forward(mixed_slot(q), mixed_g + q),
        "X": lambda m, q: mix(),
        "W": lambda m, q: weigh(),
        "D": lambda m, q: landed(),
        "E": lambda m, q: gate_block(e, 0, send=False),
        "k": lambda m, q: gather_start(hid_slot(e, q), hid_g(e, q)),
        "S": lambda m, q: share(),
        "s": lambda m, q: gather_start(shd_slot, shared_g),
        "U": lambda m, q: gather_forward(shd_slot, shared_g),
        "u": lambda m, q: own_onward(0, 0, q),
        "c": lambda m, q: own_across(q),
        "Y": lambda m, q: down_block(e, 0),
        "C": lambda m, q: shared_down(),
        "m": lambda m, q: mixer_tile(q),
    }

    def table(names, r, k, unroll):
        found = jnp.int32(-1)
        for at, name in enumerate(names):
            if at % unroll == k and name != "--":
                found = jnp.where(r == at // unroll, int(name[0]) * pieces + int(name[1]), found)
        return found

    def due(part, r, k=0, unroll=1):
        for at, what in part.items():
            if at % unroll == k:

                @pl.when(r == at // unroll)
                def _():
                    for one in what:
                        acts[one[0]](int(one[1]), int(one[2]))

    def down_tiles(weight, hidden, place):
        part = hid.shape[-1]
        for c in range(chans // TILE):
            at = slice(c * TILE, (c + 1) * TILE)
            total = dot32(hidden(0), dw[0:part, at])
            for lane in range(1, n_tp):
                total += dot32(hidden(lane), dw[lane * part : (lane + 1) * part, at])
            place(at, (weight * total).astype(jnp.bfloat16))

    def down_piece(j, q):
        with jax.named_scope("hid_wait"):
            gather_finish(hid_slot(j, q), hid_g(j, q))

        def place(at, found):
            res[j, q, :, at] = found

        with jax.named_scope("down"):
            down_tiles(wcol[j, q][:, 0:1], lambda lane: hid[j, q, lane], place)
        for h in range(SUB):
            hop(j, q, h).start()

    def down_block(j, q):
        with jax.named_scope("hid_wait"):
            for q in range(pieces):
                gather_finish(hid_slot(j, q), hid_g(j, q))

        def place(at, found):
            res[j, :, :, at] = found.reshape(pieces, part_rows, TILE)

        with jax.named_scope("down"):
            down_tiles(
                wcol[j].reshape(rows, wcol.shape[-1])[:, 0:1],
                lambda lane: hid[j, :, lane].reshape(rows, hid.shape[-1]),
                place,
            )

    def gate_block(j, q, send=True):
        with jax.named_scope("gate_wait"):
            for q in range(pieces):
                gather_finish(tok_slot(j, q), j * pieces + q)

        with jax.named_scope("gate"):
            block = tok[j].reshape(rows, width)
            made = silu_product(dot32(block, gw[...]), dot32(block, uw[...]))
            made = made.reshape(n_tp, pieces, PIECE, made.shape[-1])
            for q in range(pieces):
                hid[j, q, t] = made[:, q].reshape(part_rows, made.shape[-1])
                if send:
                    gather_start(hid_slot(j, q), hid_g(j, q))

    def gate_piece(j, q):
        with jax.named_scope("gate_wait"):
            gather_finish(tok_slot(j, q), j * pieces + q)

        with jax.named_scope("gate"):
            block = tok[j, :, q].reshape(part_rows, width)
            hid[j, q, t] = silu_product(dot32(block, gw[...]), dot32(block, uw[...]))
            gather_start(hid_slot(j, q), hid_g(j, q))

    def run(plan, unroll, gate, down):
        def step(r, _):
            for k in range(unroll):
                with jax.named_scope("pre_down"):
                    due(plan["before_down"], r, k, unroll)
                if any(name != "--" for name in plan["downs"][k::unroll]):
                    down_at = table(plan["downs"], r, k, unroll)

                    @pl.when(down_at >= 0)
                    def _():
                        down(block_at(down_at // pieces), down_at % pieces)

                with jax.named_scope("pre_gate"):
                    due(plan["before_gate"], r, k, unroll)
                gate_at = table(plan["gates"], r, k, unroll)

                @pl.when(gate_at >= 0)
                def _():
                    gate(block_at(gate_at // pieces), gate_at % pieces)

                due(plan["after_gate"], r, k, unroll)

            return 0

        lax.fori_loop(0, -(-len(plan["gates"]) // unroll), step, 0)

    @pl.when(~inner)
    def _():
        run(END_PLAN, STEPS, gate_piece, down_piece)

    @pl.when(inner)
    def _():
        run(INNER_PLAN, 1, gate_block, down_block)

    for here, after in ((~inner, END_AFTER), (inner, INNER_AFTER)):

        @pl.when(here)
        def _():
            for one in after:
                acts[one[0]](int(one[1]), int(one[2]))

    def combine(q, _):
        with jax.named_scope("final_wait"):
            for here, slot in ((e > 0, e), (e < last, n_ep)):

                @pl.when(here)
                def _():
                    for h in range(SUB):
                        hop_arrives(slot, q, h)

        total = acc[:, q].reshape(part_rows, chans)
        for found in (res[e, q], pin[e, q], pin[n_ep, q]):
            total += found.astype(jnp.float32)
        whole = total.astype(jnp.bfloat16)
        for lane in range(n_tp):
            at = pl.ds(pl.multiple_of(lane * lane_rows + q * PIECE, PIECE), PIECE)
            exp_out[at, :] = whole[lane * PIECE : (lane + 1) * PIECE]
        return 0

    lax.fori_loop(0, pieces, combine, 0)

    @pl.when(e < last)
    def _():
        halo_copy().wait_send()

    def sent(ref, sem):
        remote(ref, ref, sem, h_sem.at[1], e, partner).wait_send()

    with jax.named_scope("drain"):

        @pl.when(~inner)
        def _():
            sent(tok.at[0, 0:n_x], z_send.at[0])

        @pl.when(inner)
        def _():
            sent(tok.at[0:2, 0], z_send.at[0])
            sent(tok.at[0 : n_ep - 2, 0], z_send.at[1])
            sent(tok.at[0, 0:n_x], z_send.at[2])

        sent(tok.at[0 : n_ep - 1, 0 : n_x - 1], x_send.at[0])
        sent(tok.at[:, 0:n_x], p_send.at[0])
        sent(hid.at[:, :, 0 : n_x - 1], x_send.at[1])
        sent(hid.at[:, :, 0:n_x], p_send.at[1])
        sent(shd.at[0 : n_x - 1], x_send.at[2])
        sent(shd.at[0:n_x], p_send.at[2])
        sent(mixed.at[0 : n_x - 1], x_send.at[3])
        sent(mixed.at[0:n_x], p_send.at[3])
        sent(res.at[0 : n_ep - 1], r_send.at[0])
        sent(wts.at[0 : n_ep - 1], w_send.at[0])


def joined(n_ep, n_tp, *args):
    (og, ig, va, taps, mw, ei, ng, ids, rw, gw, uw, dw, sg, su, sd) = args
    gw, uw, dw, ng = gw[0], uw[0], dw[0], ng[None]
    bf, f32 = jnp.bfloat16, jnp.float32
    rows, chans = og.shape
    lane_rows, width = ei.shape
    n_x = n_tp // CORES
    pieces = lane_rows // PIECE
    sems = 2 * n_ep * pieces + 1 + CHUNKS
    big = (og, ig, va, taps, mw, ei, ng, gw, uw, dw, sg, su, sd)
    out = pltpu.VMEM((rows, chans), bf)
    vmem = pl.BlockSpec(memory_space=pltpu.VMEM)
    dma = pltpu.SemaphoreType.DMA
    return pl.pallas_call(
        functools.partial(kernel, n_ep, n_tp),
        out_shape=(out, out),
        in_specs=[pl.BlockSpec(memory_space=pl.ANY)] * (2 + len(big)),
        out_specs=(vmem, vmem),
        scratch_shapes=[pltpu.VMEM(a.shape, a.dtype) for a in (*big, ids.T, rw.T)]
        + [
            pltpu.VMEM((n_ep, n_tp, pieces, PIECE, width), bf),
            pltpu.VMEM((n_ep, pieces, n_tp, n_tp * PIECE, gw.shape[-1]), bf),
            pltpu.VMEM((n_tp, rows, sg.shape[-1]), bf),
            pltpu.VMEM((n_tp, rows, chans), bf),
            pltpu.VMEM((rows, chans), bf),
            pltpu.VMEM((16, chans), bf),
            pltpu.VMEM((n_ep, pieces, n_tp * PIECE, chans), bf),
            pltpu.VMEM((n_ep + 1, pieces, n_tp * PIECE, chans), bf),
            pltpu.VMEM((n_tp, pieces, PIECE, chans), f32),
            pltpu.VMEM((n_ep, pieces, n_tp * PIECE, 128), f32),
            pltpu.VMEM((n_ep, -(-n_ep // 8) * 8, -(-rows // 128) * 128), f32),
            dma((len(big) + 1 + pieces,)),
            dma((3,)),
            dma((n_x, n_ep, pieces)),
            dma((4,)),
            dma((sems, max(1, n_x - 1))),
            dma((4,)),
            dma((sems, n_x)),
            dma((1,)),
            dma((n_ep + 1, pieces, SUB)),
            dma((1,)),
            dma((n_ep,)),
            dma((2,)),
        ],
        compiler_params=pltpu.CompilerParams(
            collective_id=0, has_side_effects=True, vmem_limit_bytes=60 * 1024 * 1024
        ),
    )(ids.T, rw.T, *big)


def local(*args):
    n_ep, n_tp = lax.axis_size("ep"), lax.axis_size("tp")
    chans, lane_rows = args[0].shape[1], args[5].shape[0]
    aligned = (
        n_tp % CORES == 0
        and n_ep == 2 * ROLES
        and lane_rows == STEPS * PIECE
        and chans == MIX_TILES * TILE
        and lane_rows % PIECE == 0
        and lane_rows * n_tp == args[0].shape[0]
        and chans % TILE == 0
        and args[0].shape[0] % (16 * CHUNKS) == 0
        and args[9].shape[2] % 128 == 0
        and args[12].shape[1] % 128 == 0
    )
    return joined(n_ep, n_tp, *args) if aligned else plain(*args)


def solution(mesh):
    placed = (
        P(("grp", "ep"), "tp"),
        P(("grp", "ep"), "tp"),
        P(("grp", "ep"), "tp"),
        P(None, "tp"),
        P(None, "tp"),
        P(("grp", "ep", "tp"), None),
        P(),
        P(("grp", "ep"), None),
        P(("grp", "ep"), None),
        P("ep", None, "tp"),
        P("ep", None, "tp"),
        P("ep", None, "tp"),
        P(None, "tp"),
        P(None, "tp"),
        P(None, "tp"),
    )
    return jax.shard_map(
        local,
        mesh=mesh,
        in_specs=placed,
        out_specs=(P(("grp", "ep"), "tp"), P(("grp", "ep"), "tp")),
        check_vma=False,
    )
```
